256 devices in a mesh: ep: 64 (over z, x, core), tp: 4 (over y).
Axes of the slice: x: 4, y: 4, z: 8, core: 2. Of those that a mesh axis runs over, the one named last changes fastest.
Arguments:
- tokens: bfloat16 [2048, 2048], P('ep'), may hold values from -6 to 6
- norm_gain_attn: float32 [2048], replicated, may hold values from 0.1 to 1.9
- w_query: bfloat16 [2048, 2048], P('ep', 'tp'), may hold values from -0.125 to 0.125
- w_key: bfloat16 [2048, 256], P('ep', 'tp'), may hold values from -0.125 to 0.125
- w_value: bfloat16 [2048, 256], P('ep', 'tp'), may hold values from -0.125 to 0.125
- w_forget: bfloat16 [2048, 32], P(None, 'tp'), may hold values from -0.125 to 0.125
- forget_bias: float32 [32], P('tp'), may hold values from -1 to 3
- cache_keys: bfloat16 [2048, 256, 1024], P('ep', 'tp'), may hold values from -64 to 64
- cache_values: bfloat16 [2048, 256, 1024], P('ep', 'tp'), may hold values from -6 to 6
- cache_logcum: float32 [2048, 32, 1024], P('ep', 'tp'), may hold values from -2048 to 0, as said below
- lengths: int32 [2048], P('ep'), may hold values from 1 to 1023, as said below
- w_out: bfloat16 [2048, 2048], P('tp'), may hold values from -0.125 to 0.125
- norm_gain_mix: float32 [2048], replicated, may hold values from 0.1 to 1.9
- norm_gain_ffn: float32 [2048], replicated, may hold values from 0.1 to 1.9
- expert_gate: bfloat16 [2048, 65536], P(None, ('ep', 'tp')), may hold values from -0.125 to 0.125
- expert_up: bfloat16 [2048, 65536], P(None, ('ep', 'tp')), may hold values from -0.125 to 0.125
- expert_down: bfloat16 [65536, 2048], P(('ep', 'tp')), may hold values from -0.09375 to 0.09375
- routes: int32 [2048, 2], P('ep'), may hold values from 0 to 15, all different within a row; in each aligned block of 32 rows (0 to 31, 32 to 63, ...) at most 8 rows name the same one
- route_weights: float32 [2048, 2], P('ep'), may hold values from 0.2 to 1
Outputs:
- layer_out: bfloat16 [2048, 2048], P('ep', 'tp')
- new_keys: bfloat16 [2048, 256], P('ep', 'tp')
- new_values: bfloat16 [2048, 256], P('ep', 'tp')
- new_log_gate: float32 [2048, 32], P('ep', 'tp')
The draws below stay inside these ranges and needn't reach their ends.
Inputs may be any that keep to these rules, and one draw needn't show every extreme that they name: `routes`: each row names 2 different experts. Within the rows of one index of ep no expert is named by more than 8 rows, and in every draw some expert is named by exactly 8 rows of some index. `lengths`: some sequence has 1023 cached positions in every draw. `cache_logcum`: never rising along positions (the last dimension).
All inputs are finite; a program needn't handle non-finite values.
Results may differ from the reference program's by a relative error of at most 0.013.
Values may be sent and summed in bfloat16 or wider, within the bound.
A program may use at most 64 MiB of HBM per device.

```python
import math
import jax
import jax.numpy as jnp
import numpy as np
from jax import lax

D = 2048
HEAD_TOTAL = 32
KV_HEADS = 4
HEAD_DIM = 64
FF = 4096
TOP = 2
B_DEV = 32
LENGTH_LIMIT = 1024
SEQUENCE_TOTAL = 2048
EXPERTS = 16
CAP = 8
N_TP = 4


def draw_cache_logcum(key, part):
    gathered_keys = jax.random.split(key, 5)
    fast_share = 0.5
    fast_heads = jax.random.uniform(gathered_keys[0], (HEAD_TOTAL,)) < fast_share
    head_rate = jnp.where(fast_heads, 0.1, 0.5 / LENGTH_LIMIT)
    seq_factor = jnp.exp(jax.random.uniform(gathered_keys[1], (SEQUENCE_TOTAL, 1, 1), minval=-0.7, maxval=0.7))
    rough_factor = jnp.exp(jax.random.uniform(gathered_keys[2], (SEQUENCE_TOTAL, LENGTH_LIMIT, HEAD_TOTAL), minval=-0.7, maxval=0.7))
    decode_step_gates = -head_rate[None, None, :] * seq_factor * rough_factor
    spike_positions = jax.random.uniform(gathered_keys[3], (SEQUENCE_TOTAL, LENGTH_LIMIT, 1)) < 2.0 / LENGTH_LIMIT
    spike_penalty = jax.random.uniform(gathered_keys[4], (SEQUENCE_TOTAL, LENGTH_LIMIT, HEAD_TOTAL), minval=0.22, maxval=0.69)
    decode_step_gates = decode_step_gates - jnp.where(spike_positions, spike_penalty, 0.0)
    summed = jnp.cumsum(decode_step_gates, axis=1)
    return jnp.transpose(summed, (0, 2, 1)).astype(jnp.float32)


def draw_cache_keys(key, part):
    gathered_keys = jax.random.split(key, 1)
    shape_full = (SEQUENCE_TOTAL, LENGTH_LIMIT, KV_HEADS * HEAD_DIM)
    result = jnp.clip(jax.random.normal(gathered_keys[0], shape_full), -6.0, 6.0)
    return jnp.transpose(result, (0, 2, 1)).astype(jnp.bfloat16)


def draw_lengths(key, part):
    gathered_keys = jax.random.split(key, 3)
    block_tops = jax.random.randint(gathered_keys[0], (SEQUENCE_TOTAL // B_DEV, 1), LENGTH_LIMIT // 8, LENGTH_LIMIT)
    raw_draws = jax.random.randint(gathered_keys[1], (SEQUENCE_TOTAL // B_DEV, B_DEV), 0, LENGTH_LIMIT)
    seq_lengths = (1 + raw_draws % block_tops).reshape(-1)
    chosen = jax.random.randint(gathered_keys[2], (), 0, SEQUENCE_TOTAL)
    seq_lengths = seq_lengths.at[chosen].set(LENGTH_LIMIT - 1)
    return seq_lengths.astype(jnp.int32)


def block_levels(rng, dims, pieces, least, largest):
    def one(dim, shards_of):
        draws = jax.random.uniform(jax.random.fold_in(jax.random.fold_in(rng, 6), dim), (shards_of,), jnp.float32, least / len(pieces), largest / len(pieces))
        return jnp.repeat(jnp.exp(draws), dims[dim] // shards_of).reshape((-1,) + (1,) * (len(dims) - dim - 1))

    loudness = one(*pieces[0])
    for cut in pieces[1:]:
        loudness = loudness * one(*cut)
    return loudness


def assign_block(rng, own, number, rows, number_of, top, bound, lean):
    ranking = jax.random.permutation(rng, number_of)
    heavy_load, common = shares(number_of, rows * top, bound, lean, True), shares(number_of, rows * top, bound, lean, False)
    places = jnp.arange(number_of)

    def named(sizes, rotation):
        used = int((sizes > 0).sum())
        fixed = max(1, used // 4)
        passed = fixed + (places - fixed + rotation * (used - fixed)) % max(1, number_of - fixed)
        return jnp.zeros((number_of,), jnp.int32).at[ranking[jnp.where(places < fixed, places, passed)]].set(jnp.asarray(sizes, jnp.int32))

    sizes = jnp.where(number % 4 == 0, named(heavy_load, number // 4), named(common, number - number // 4 - 1))
    mixed = jax.random.permutation(jax.random.fold_in(own, 3), number_of)
    donor, receiver = mixed[0:number_of // 2 * 2:2], mixed[1:number_of // 2 * 2:2]
    margin = jnp.minimum(sizes[donor] - 1, bound - sizes[receiver]) // 2
    margin = jnp.where((donor == ranking[0]) | (receiver == ranking[0]) | (sizes[receiver] == 0), 0, jnp.maximum(margin, 0))
    passed = jax.random.randint(jax.random.fold_in(own, 4), (number_of // 2,), 0, 1 << 20) % (margin + 1)
    sizes = sizes.at[donor].add(-passed).at[receiver].add(passed)
    labels = jnp.searchsorted(jnp.cumsum(sizes), jnp.arange(rows * top), side="right").astype(jnp.int32)
    grid = labels.reshape(top, rows).T
    grid = grid[jax.random.permutation(jax.random.fold_in(own, 1), rows)]
    rotation = jax.random.randint(jax.random.fold_in(own, 2), (rows, 1), 0, top)
    return jnp.take_along_axis(grid, (jnp.arange(top)[None, :] + rotation) % top, axis=1)


def shares(count, total, bound, lean, full):
    loads = [(1 << 20) // math.isqrt(rank ** lean) + 1 for rank in range(1, count + 1)]
    largest = bound if full else min(bound, max(-(-total // count), total * loads[0] // sum(loads)))
    least = 1 if total - largest >= count - 1 else 0
    holding, rest = [largest] + [least] * (count - 1), total - largest - least * (count - 1)
    while rest > 0:
        candidates = [i for i in range(1, count) if holding[i] < largest] or [i for i in range(1, count) if holding[i] < bound]
        pool, remaining = sum([loads[i] for i in candidates]), rest
        for i in candidates:
            addition = min(bound - holding[i], max(1, remaining * loads[i] // pool), rest)
            holding[i] = holding[i] + addition
            rest = rest - addition
    return np.array(holding)


def bell_draw(rng, shape, width, most, cuts=(), kind=jnp.bfloat16):
    level = block_levels(rng, shape, cuts, -0.22, 0.18) if cuts else 1.0
    values = jax.random.normal(rng, shape, jnp.float32) * width * level
    return jnp.minimum(jnp.maximum(values, -most), most).astype(kind)


def setup_inputs(seed: int = 0) -> dict:
    streams_of = jax.random.split(jax.random.key(seed), 20)
    tokens = bell_draw(streams_of[0], (SEQUENCE_TOTAL, D), 1.0, 6.0, ((0, 64),))
    norm_gain_attn = jnp.clip(1.0 + 0.18 * jax.random.normal(streams_of[1], (D,), jnp.float32), 0.1, 1.9)
    w_query = bell_draw(streams_of[2], (D, HEAD_TOTAL * HEAD_DIM), D ** -0.5, 0.125, ((0, 64), (1, 4)))
    w_key = bell_draw(streams_of[3], (D, KV_HEADS * HEAD_DIM), D ** -0.5, 0.125, ((0, 64), (1, 4)))
    w_value = bell_draw(streams_of[4], (D, KV_HEADS * HEAD_DIM), D ** -0.5, 0.125, ((0, 64), (1, 4)))
    w_forget = bell_draw(streams_of[5], (D, HEAD_TOTAL), D ** -0.5, 0.125, ((1, 4),))
    forget_bias = jnp.clip(-1.0 + 4.0 * jax.random.uniform(streams_of[6], (HEAD_TOTAL,), jnp.float32) ** block_levels(streams_of[6], (HEAD_TOTAL,), ((0, 4),), -0.2, 0.2), -1.0, 3.0)
    cache_keys = draw_cache_keys(jax.random.fold_in(streams_of[19], 71), 0)
    cache_values = bell_draw(streams_of[8], (SEQUENCE_TOTAL, KV_HEADS * HEAD_DIM, LENGTH_LIMIT), 1.0, 6.0, ((0, 64), (1, 4)))
    cache_logcum = draw_cache_logcum(jax.random.fold_in(streams_of[19], 71), 0)
    lengths = draw_lengths(jax.random.fold_in(streams_of[19], 71), 0)
    w_out = bell_draw(streams_of[11], (HEAD_TOTAL * HEAD_DIM, D), (HEAD_TOTAL * HEAD_DIM) ** -0.5, 0.125, ((0, 4),))
    norm_gain_mix = jnp.clip(1.0 + 0.18 * jax.random.normal(streams_of[12], (D,), jnp.float32), 0.1, 1.9)
    norm_gain_ffn = jnp.clip(1.0 + 0.18 * jax.random.normal(streams_of[13], (D,), jnp.float32), 0.1, 1.9)
    expert_gate = bell_draw(streams_of[14], (D, EXPERTS * FF), D ** -0.5, 0.125, ((1, 256),))
    expert_up = bell_draw(streams_of[15], (D, EXPERTS * FF), D ** -0.5, 0.125, ((1, 256),))
    expert_down = bell_draw(streams_of[16], (EXPERTS * FF, D), FF ** -0.5, 0.09375, ((0, 256),))
    routes_keys = jax.random.split(jax.random.fold_in(streams_of[17], 1), SEQUENCE_TOTAL // B_DEV)
    routes_turns = jax.random.permutation(jax.random.fold_in(streams_of[17], 3), SEQUENCE_TOTAL // B_DEV)
    routes = jax.vmap(lambda own, number: assign_block(jax.random.fold_in(streams_of[17], 2), own, number, B_DEV, EXPERTS, TOP, CAP, 2))(routes_keys, routes_turns).reshape((SEQUENCE_TOTAL, TOP))
    route_weights = jnp.clip(jnp.exp(math.log(1.0) - 1.609438 * jax.random.uniform(streams_of[18], (SEQUENCE_TOTAL, TOP), jnp.float32) ** block_levels(streams_of[18], (SEQUENCE_TOTAL, TOP), ((0, 64),), -0.2, 0.2)), 0.2, 1.0)
    return dict(tokens=tokens, norm_gain_attn=norm_gain_attn, w_query=w_query, w_key=w_key, w_value=w_value, w_forget=w_forget, forget_bias=forget_bias, cache_keys=cache_keys, cache_values=cache_values, cache_logcum=cache_logcum, lengths=lengths, w_out=w_out, norm_gain_mix=norm_gain_mix, norm_gain_ffn=norm_gain_ffn, expert_gate=expert_gate, expert_up=expert_up, expert_down=expert_down, routes=routes, route_weights=route_weights)


EPSILON = 1e-06
MASKED = -1e+30

def rms_scaled(field, gain_vector):
    return field * lax.rsqrt(lax.optimization_barrier(jnp.mean(field * field, axis=-1, keepdims=True)) + EPSILON) * gain_vector

def attend(query, new_key, new_value, log_gate, key_cache, value_cache, logcum, seq_lengths):
    count = query.shape[0]
    scale = HEAD_DIM ** (-0.5)
    group = HEAD_TOTAL // KV_HEADS
    query_heads = query.astype(jnp.float32).reshape(count, KV_HEADS, group, HEAD_DIM)
    key_heads = key_cache.astype(jnp.float32).reshape(count, KV_HEADS, HEAD_DIM, LENGTH_LIMIT)
    value_heads = value_cache.astype(jnp.float32).reshape(count, KV_HEADS, HEAD_DIM, LENGTH_LIMIT)
    scores = jnp.einsum('bkgd,bkdl->bkgl', query_heads, key_heads).reshape(count, HEAD_TOTAL, LENGTH_LIMIT) * scale
    own_key = new_key.astype(jnp.float32).reshape(count, KV_HEADS, 1, HEAD_DIM)
    own_score = lax.optimization_barrier(jnp.sum(query_heads * own_key, axis=-1)).reshape(count, HEAD_TOTAL) * scale
    index = jnp.broadcast_to((seq_lengths - 1).astype(jnp.int32)[:, None, None], (count, HEAD_TOTAL, 1))
    last_cum = jnp.take_along_axis(logcum, index, axis=2)[:, :, 0]
    shift = (last_cum + log_gate)[:, :, None] - logcum
    places = jnp.arange(LENGTH_LIMIT, dtype=jnp.int32)
    valid = (places[None, :] < seq_lengths[:, None])[:, None, :]
    past = jnp.where(valid, scores + shift, MASKED)
    peak = jnp.maximum(lax.optimization_barrier(jnp.max(past, axis=-1)), own_score)
    past_exp = jnp.exp(past - peak[:, :, None])
    own_exp = jnp.exp(own_score - peak)
    total = lax.optimization_barrier(jnp.sum(past_exp, axis=-1)) + own_exp
    past_weight = lax.optimization_barrier((past_exp / total[:, :, None]).astype(jnp.bfloat16)).astype(jnp.float32)
    own_weight = lax.optimization_barrier((own_exp / total).astype(jnp.bfloat16)).astype(jnp.float32)
    past_weight = past_weight.reshape(count, KV_HEADS, group, LENGTH_LIMIT)
    mixed = jnp.einsum('bkgl,bkdl->bkgd', past_weight, value_heads)
    own_value = new_value.astype(jnp.float32).reshape(count, KV_HEADS, 1, HEAD_DIM)
    mixed = mixed + own_weight.reshape(count, KV_HEADS, group)[:, :, :, None] * own_value
    return mixed.astype(jnp.bfloat16).reshape(count, HEAD_TOTAL * HEAD_DIM)

def reference(tokens, norm_gain_attn, w_query, w_key, w_value, w_forget, forget_bias, cache_keys, cache_values, cache_logcum, lengths, w_out, norm_gain_mix, norm_gain_ffn, expert_gate, expert_up, expert_down, routes, route_weights):
    residual = tokens.astype(jnp.float32)
    normed = rms_scaled(residual, norm_gain_attn).astype(jnp.bfloat16)
    query = jnp.dot(normed, w_query, preferred_element_type=jnp.float32).astype(jnp.bfloat16)
    new_keys = jnp.dot(normed, w_key, preferred_element_type=jnp.float32).astype(jnp.bfloat16)
    new_values = jnp.dot(normed, w_value, preferred_element_type=jnp.float32).astype(jnp.bfloat16)
    new_log_gate = jax.nn.log_sigmoid(jnp.dot(normed, w_forget, preferred_element_type=jnp.float32) + forget_bias)
    groups = SEQUENCE_TOTAL // B_DEV

    def by_group(array):
        return array.reshape((groups, B_DEV) + array.shape[1:])

    def one_group(items):
        return attend(*items)
    heads_out = lax.map(one_group, (by_group(query), by_group(new_keys), by_group(new_values), by_group(new_log_gate), by_group(cache_keys), by_group(cache_values), by_group(cache_logcum), by_group(lengths)))
    heads_out = heads_out.reshape(SEQUENCE_TOTAL, HEAD_TOTAL * HEAD_DIM)
    head_width = HEAD_TOTAL * HEAD_DIM // N_TP
    grouped_out = heads_out.astype(jnp.float32).reshape(SEQUENCE_TOTAL, N_TP, head_width)
    grouped_w = w_out.astype(jnp.float32).reshape(N_TP, head_width, D)
    partials = jnp.einsum('stc,tcd->tsd', grouped_out, grouped_w)
    partials = lax.optimization_barrier(partials.astype(jnp.bfloat16)).astype(jnp.float32)
    mix = lax.optimization_barrier(jnp.sum(partials, axis=0))
    mixed_res = residual + rms_scaled(mix, norm_gain_mix)
    ffn_in = rms_scaled(mixed_res, norm_gain_ffn).astype(jnp.bfloat16)

    def expert_step(carry, expert_index):
        start = expert_index * FF
        gate_part = jnp.dot(ffn_in, lax.dynamic_slice_in_dim(expert_gate, start, FF, 1), preferred_element_type=jnp.float32)
        up_part = jnp.dot(ffn_in, lax.dynamic_slice_in_dim(expert_up, start, FF, 1), preferred_element_type=jnp.float32)
        hidden = (jax.nn.silu(gate_part) * up_part).astype(jnp.bfloat16)
        expert_out = jnp.dot(hidden, lax.dynamic_slice_in_dim(expert_down, start, FF, 0), preferred_element_type=jnp.float32)
        weight = lax.optimization_barrier(jnp.sum(jnp.where(routes == expert_index, route_weights, 0.0), axis=1))
        return (carry + weight[:, None] * expert_out, None)
    routed, _ = lax.scan(expert_step, jnp.zeros((SEQUENCE_TOTAL, D), jnp.float32), jnp.arange(EXPERTS, dtype=jnp.int32))
    layer_out = (mixed_res + routed).astype(jnp.bfloat16)
    return (layer_out, new_keys, new_values, new_log_gate)
```

```python
import functools

import jax
import jax.numpy as jnp
from jax import lax
from jax.experimental import pallas as pl
from jax.experimental.pallas import tpu as pltpu
from jax.sharding import PartitionSpec as P

HEAD_TOTAL = 32
KV_HEADS = 4
HEAD_DIM = 64
NX = 4
NC = 2
SLOTS = 8
EPSILON = 1e-06
MASKED = -1e30
MESH = pl.DeviceIdType.MESH
F32 = jnp.float32
BF16 = jnp.bfloat16


def rms_scaled(field, gain_vector):
    return (
        field * lax.rsqrt(jnp.mean(field * field, axis=-1, keepdims=True) + EPSILON) * gain_vector
    )


def place():
    ep, y = lax.axis_index("ep"), lax.axis_index("tp")
    z = lax.div(ep, NX * NC)
    within = lax.rem(ep, NX * NC)
    return ep, y, z, lax.div(within, NC), lax.rem(within, NC)


def remote(src, dst, send, recv, ep, y):
    return pltpu.make_async_remote_copy(
        src_ref=src, dst_ref=dst, send_sem=send, recv_sem=recv, device_id=(ep, y), device_id_type=MESH
    )


def project_kernel(
    nz, tokens, gain, w_own, out, normed, t_in, w_in, sums, p_out, p_in, t_send, t_recv, w_send, w_recv, p_send, p_recv
):
    _, y, z, x, c = place()
    flat = NX * NC
    at = x * NC + c
    barrier = pltpu.get_barrier_semaphore()

    def z_peer(d):
        return lax.rem(z + d, nz) * flat + at

    def row_peer(d):
        return z * flat + lax.rem(at + d, flat)

    for d in range(1, nz):
        pl.semaphore_signal(barrier, inc=1, device_id=(z_peer(d), y), device_id_type=MESH)
    for d in range(1, flat):
        pl.semaphore_signal(barrier, inc=1, device_id=(row_peer(d), y), device_id_type=MESH)
    scaled = rms_scaled(tokens[...].astype(F32), gain[...]).astype(BF16)
    width = scaled.shape[1] // nz
    for k in range(nz):
        normed[k] = scaled[:, k * width : (k + 1) * width]
    pl.semaphore_wait(barrier, nz - 1 + flat - 1)

    far_first = sorted(range(1, nz), key=lambda d: -min(d, nz - d))
    w_copies = [
        remote(w_own, w_in.at[at], w_send.at[d], w_recv.at[d], row_peer(d), y) for d in range(1, flat)
    ]
    t_copies = [
        remote(normed.at[lax.rem(z + d, nz)], t_in.at[d], t_send.at[d], t_recv.at[d], z_peer(d), y)
        for d in far_first
    ]
    for copy in w_copies:
        copy.start()
    for copy in t_copies:
        copy.start()
    w_in[at] = w_own[...]
    t_in[0] = normed[z]
    for copy in w_copies + t_copies:
        copy.wait_recv()
    rows = tokens.shape[0]
    weights = w_in[...].reshape(flat * w_own.shape[0], w_own.shape[1])
    product = jnp.dot(t_in[...].reshape(nz * rows, width), weights, preferred_element_type=F32)
    for d in range(1, nz):
        p_out[d] = product[d * rows : (d + 1) * rows].astype(BF16)
    p_copies = [
        remote(p_out.at[d], p_in.at[d], p_send.at[d], p_recv.at[d], z_peer(nz - d), y) for d in far_first
    ]
    for copy in p_copies:
        copy.start()
    sums[...] = product[:rows]
    for copy in w_copies + t_copies:
        copy.wait_send()
    for copy in sorted(range(len(p_copies)), key=lambda i: -i):
        p_copies[copy].wait_recv()
    total = sums[...]
    for d in range(1, nz):
        total = total + p_in[d].astype(F32)
    out[...] = total
    for copy in p_copies:
        copy.wait_send()


def project(nz, tokens, gain, w_own):
    rows, width = tokens.shape
    cols = w_own.shape[1]
    flat = NX * NC
    vmem = pl.BlockSpec(memory_space=pltpu.VMEM)
    dma = pltpu.SemaphoreType.DMA
    return pl.pallas_call(
        functools.partial(project_kernel, nz),
        out_shape=jax.ShapeDtypeStruct((rows, cols), F32),
        in_specs=[vmem] * 3,
        out_specs=vmem,
        scratch_shapes=[
            pltpu.VMEM((nz, rows, width // nz), BF16),
            pltpu.VMEM((nz, rows, width // nz), BF16),
            pltpu.VMEM((flat, w_own.shape[0], cols), BF16),
            pltpu.VMEM((rows, cols), F32),
            pltpu.VMEM((nz, rows, cols), BF16),
            pltpu.VMEM((nz, rows, cols), BF16),
            dma((nz,)),
            dma((nz,)),
            dma((flat,)),
            dma((flat,)),
            dma((nz,)),
            dma((nz,)),
        ],
        compiler_params=pltpu.CompilerParams(collective_id=0, has_side_effects=True),
        name="project",
    )(tokens, gain, w_own)


def slotted(routes, weights, expert_of, slot_of, axis):
    first, second = routes
    in_first, in_second = first == expert_of, second == expert_of
    member = jnp.where(in_first | in_second, 1.0, 0.0).astype(F32)
    rows = member.shape[axis]
    row = lax.broadcasted_iota(jnp.int32, (rows, rows), 0)
    col = lax.broadcasted_iota(jnp.int32, (rows, rows), 1)
    if axis == 0:
        before = jnp.where(col < row, 1.0, 0.0).astype(BF16)
        earlier = jnp.dot(before, member.astype(BF16), preferred_element_type=F32)
    else:
        before = jnp.where(row < col, 1.0, 0.0).astype(BF16)
        earlier = jnp.dot(member.astype(BF16), before, preferred_element_type=F32)
    chosen = jnp.where(earlier == slot_of.astype(F32), member, 0.0)
    if weights is None:
        return chosen
    return chosen * (jnp.where(in_first, weights[0], 0.0) + jnp.where(in_second, weights[1], 0.0))


def experts_kernel(
    nz,
    ny,
    heads,
    tokens,
    gain_mix,
    gain_ffn,
    routes,
    routes_across,
    route_weights,
    w_out,
    gate,
    up,
    down,
    out,
    wo_v,
    gate_v,
    up_v,
    down_v,
    mix_out,
    mix_in,
    mixed_res,
    packed,
    z_in,
    x_in,
    share_out,
    share_in,
    back_out,
    back_in,
    load_sem,
    pair_send,
    pair_recv,
    y_send,
    y_recv,
    z_send,
    z_recv,
    x_send,
    x_recv,
    s_send,
    s_recv,
    b_send,
    b_recv,
):
    ep, y, z, x, c = place()
    flat = NX * NC
    rows, width = tokens.shape
    part = width // ny
    barrier = pltpu.get_barrier_semaphore()

    def chip(dz, dx):
        return lax.rem(z + dz, nz) * flat + lax.rem(x + dx, NX) * NC + c

    def signal(ep_to, y_to):
        pl.semaphore_signal(barrier, inc=1, device_id=(ep_to, y_to), device_id_type=MESH)

    for dz in range(nz):
        for dx in range(NX):
            if dz or dx:
                signal(chip(dz, dx), y)
    for dy in range(1, ny):
        signal(ep, lax.rem(y + dy, ny))
    partner = ep + 1 - 2 * c
    signal(partner, y)

    loads = [
        pltpu.make_async_copy(w_out, wo_v, load_sem.at[0]),
        pltpu.make_async_copy(gate, gate_v.at[0], load_sem.at[1]),
        pltpu.make_async_copy(up, up_v.at[0], load_sem.at[2]),
        pltpu.make_async_copy(down, down_v.at[0], load_sem.at[3]),
    ]
    for load in loads:
        load.start()

    shape = (nz * 2 * SLOTS, rows)
    lane = lax.broadcasted_iota(jnp.int32, shape, 0)
    expert_of = 2 * lax.rem(z + lane // (2 * SLOTS), nz) + (lane // SLOTS) % 2
    picking = slotted(
        (routes_across[0:1, :], routes_across[1:2, :]), None, expert_of, lane % SLOTS, 1
    ).astype(BF16)
    shape = (rows, nz * NX * SLOTS)
    lane = lax.broadcasted_iota(jnp.int32, shape, 1)
    expert_of = 2 * lax.rem(z + lane // (NX * SLOTS), nz) + lax.rem(x + (lane // SLOTS) % NX, NX) // 2
    weighing = slotted(
        (routes[:, 0:1], routes[:, 1:2]),
        (route_weights[:, 0:1], route_weights[:, 1:2]),
        expert_of,
        lane % SLOTS,
        0,
    )

    loads[0].wait()
    mix_out[...] = jnp.dot(heads[...], wo_v[...], preferred_element_type=F32).astype(BF16)
    pl.semaphore_wait(barrier, nz * NX - 1 + ny - 1 + 1)
    y_copies = [
        remote(mix_out, mix_in.at[d], y_send.at[d], y_recv.at[d], ep, lax.rem(y + d, ny))
        for d in range(1, ny)
    ]
    for copy in y_copies:
        copy.start()
    pair_copies = [
        remote(src, dst.at[1], pair_send.at[i], pair_recv.at[i], partner, y)
        for i, (src, dst) in enumerate(((gate, gate_v), (up, up_v), (down, down_v)))
    ]
    for copy in pair_copies:
        copy.start()
    mix = mix_out[...].astype(F32)
    for i, copy in enumerate(y_copies):
        copy.wait_recv()
        mix = mix + mix_in[i + 1].astype(F32)
    mixed = tokens[...].astype(F32) + rms_scaled(mix, gain_mix[...])
    for k in range(ny):
        mixed_res[k] = mixed[:, k * part : (k + 1) * part]
    ffn_in = rms_scaled(mixed, gain_ffn[...]).astype(BF16)
    chosen = jnp.dot(picking, ffn_in, preferred_element_type=F32).astype(BF16)
    packed[...] = chosen.reshape(nz, 2, SLOTS, width)

    order = sorted(range(1, nz), key=lambda d: min(d, nz - d))
    z_copies = {
        d: remote(packed.at[d], z_in.at[d], z_send.at[d], z_recv.at[d], chip(d, 0), y) for d in order
    }
    for d in order:
        z_copies[d].start()
    z_in[0] = packed[0]
    x_copies = []
    for d in [0, *order]:
        if d:
            z_copies[d].wait_recv()
        for dx in range(1, NX):
            half = lax.rem(x + dx, NX) // 2
            copy = remote(
                z_in.at[d, half], x_in.at[d, dx], x_send.at[d, dx], x_recv.at[d, dx], chip(0, dx), y
            )
            copy.start()
            x_copies.append(copy)
        x_in[d, 0] = z_in[d, x // 2]

    for load in loads[1:]:
        load.wait()
    for copy in pair_copies:
        copy.wait_recv()
    for copy in x_copies:
        copy.wait_recv()
    arrived = x_in[...].reshape(nz * NX * SLOTS, width)
    hidden = []
    for k in range(NC):
        gate_part = jnp.dot(arrived, gate_v[k], preferred_element_type=F32)
        up_part = jnp.dot(arrived, up_v[k], preferred_element_type=F32)
        hidden.append((gate_part / (1.0 + jnp.exp(-gate_part)) * up_part).astype(BF16))
    for j in range(ny):
        share = jnp.dot(hidden[0], down_v[0, :, j * part : (j + 1) * part], preferred_element_type=F32)
        share += jnp.dot(hidden[1], down_v[1, :, j * part : (j + 1) * part], preferred_element_type=F32)
        share_out[j] = share.astype(BF16)
    s_copies = [
        remote(
            share_out.at[lax.rem(y + d, ny)], share_in.at[d], s_send.at[d], s_recv.at[d], ep, lax.rem(y + d, ny)
        )
        for d in range(1, ny)
    ]
    for copy in s_copies:
        copy.start()
    total = share_out[y].astype(F32)
    for i, copy in enumerate(s_copies):
        copy.wait_recv()
        total = total + share_in[i + 1].astype(F32)
    back_out[...] = total.astype(BF16).reshape(nz, NX, SLOTS, part)

    b_copies = [
        remote(
            back_out.at[d, dx], back_in.at[d, dx], b_send.at[d, dx], b_recv.at[d, dx], chip(nz - d, NX - dx), y
        )
        for d in range(nz)
        for dx in range(NX)
        if d or dx
    ]
    for copy in b_copies:
        copy.start()
    back_in[0, 0] = back_out[0, 0]
    for copy in y_copies + pair_copies + list(z_copies.values()) + x_copies + s_copies:
        copy.wait_send()
    for copy in b_copies:
        copy.wait_recv()
    returned = back_in[...].reshape(nz * NX * SLOTS, part)
    coarse = weighing.astype(BF16)
    fine = (weighing - coarse.astype(F32)).astype(BF16)
    routed = jnp.dot(coarse, returned, preferred_element_type=F32)
    routed += jnp.dot(fine, returned, preferred_element_type=F32)
    out[...] = (mixed_res[y] + routed).astype(BF16)
    for copy in b_copies:
        copy.wait_send()


def experts(nz, ny, heads, tokens, gain_mix, gain_ffn, routes, route_weights, w_out, gate, up, down):
    rows, width = tokens.shape
    part = width // ny
    hidden = gate.shape[1]
    lanes = nz * NX * SLOTS
    vmem = pl.BlockSpec(memory_space=pltpu.VMEM)
    kept = pl.BlockSpec(memory_space=pl.ANY)
    dma = pltpu.SemaphoreType.DMA
    return pl.pallas_call(
        functools.partial(experts_kernel, nz, ny),
        out_shape=jax.ShapeDtypeStruct((rows, part), BF16),
        in_specs=[vmem] * 7 + [kept] * 4,
        out_specs=vmem,
        scratch_shapes=[
            pltpu.VMEM(w_out.shape, BF16),
            pltpu.VMEM((NC, width, hidden), BF16),
            pltpu.VMEM((NC, width, hidden), BF16),
            pltpu.VMEM((NC, hidden, width), BF16),
            pltpu.VMEM((rows, width), BF16),
            pltpu.VMEM((ny, rows, width), BF16),
            pltpu.VMEM((ny, rows, part), F32),
            pltpu.VMEM((nz, 2, SLOTS, width), BF16),
            pltpu.VMEM((nz, 2, SLOTS, width), BF16),
            pltpu.VMEM((nz, NX, SLOTS, width), BF16),
            pltpu.VMEM((ny, lanes, part), BF16),
            pltpu.VMEM((ny, lanes, part), BF16),
            pltpu.VMEM((nz, NX, SLOTS, part), BF16),
            pltpu.VMEM((nz, NX, SLOTS, part), BF16),
            dma((4,)),
            dma((3,)),
            dma((3,)),
            dma((ny,)),
            dma((ny,)),
            dma((nz,)),
            dma((nz,)),
            dma((nz, NX)),
            dma((nz, NX)),
            dma((ny,)),
            dma((ny,)),
            dma((nz, NX)),
            dma((nz, NX)),
        ],
        compiler_params=pltpu.CompilerParams(collective_id=1, has_side_effects=True),
        name="experts",
    )(heads, tokens, gain_mix, gain_ffn, routes, routes.T, route_weights, w_out, gate, up, down)


def body(
    nz,
    ny,
    tokens,
    norm_gain_attn,
    w_query,
    w_key,
    w_value,
    w_forget,
    forget_bias,
    cache_keys,
    cache_values,
    cache_logcum,
    lengths,
    w_out,
    norm_gain_mix,
    norm_gain_ffn,
    expert_gate,
    expert_up,
    expert_down,
    routes,
    route_weights,
):
    row_count = tokens.shape[0]
    query_cols = w_query.shape[1]
    key_cols = w_key.shape[1]
    residual = tokens.astype(F32)
    normed = rms_scaled(residual, norm_gain_attn).astype(BF16)
    projected = project(
        nz, tokens, norm_gain_attn[None, :], jnp.concatenate((w_query, w_key, w_value), axis=1)
    )
    query = projected[:, :query_cols].astype(BF16)
    new_keys = projected[:, query_cols : query_cols + key_cols].astype(BF16)
    new_values = projected[:, query_cols + key_cols :].astype(BF16)
    new_log_gate = jax.nn.log_sigmoid(
        jnp.dot(normed, w_forget, preferred_element_type=F32) + forget_bias
    )
    local_heads = query_cols // HEAD_DIM
    local_kv = key_cols // HEAD_DIM
    group = HEAD_TOTAL // KV_HEADS
    span_len = cache_keys.shape[2]
    scale = HEAD_DIM ** (-0.5)
    query_heads = query.reshape(row_count, local_kv, group, HEAD_DIM)
    key_heads = cache_keys.reshape(row_count, local_kv, HEAD_DIM, span_len)
    value_heads = cache_values.reshape(row_count, local_kv, HEAD_DIM, span_len)
    scores = jnp.einsum("bkgd,bkdl->bkgl", query_heads, key_heads, preferred_element_type=F32)
    scores = scores.reshape(row_count, local_heads, span_len) * scale
    own_key = new_keys.astype(F32).reshape(row_count, local_kv, 1, HEAD_DIM)
    own_score = (
        jnp.sum(query_heads.astype(F32) * own_key, axis=-1).reshape(row_count, local_heads) * scale
    )
    places = jnp.arange(span_len, dtype=jnp.int32)
    at_last = (places[None, :] == (lengths - 1)[:, None]).astype(F32)
    last_cum = jnp.sum(cache_logcum * at_last[:, None, :], axis=2)
    shift = (last_cum + new_log_gate)[:, :, None] - cache_logcum
    valid = (places[None, :] < lengths[:, None])[:, None, :]
    past = jnp.where(valid, scores + shift, MASKED)
    peak = jnp.maximum(jnp.max(past, axis=-1), own_score)
    past_exp = jnp.exp(past - peak[:, :, None])
    own_exp = jnp.exp(own_score - peak)
    total = jnp.sum(past_exp, axis=-1) + own_exp
    past_weight = (
        (past_exp / total[:, :, None]).astype(BF16).reshape(row_count, local_kv, group, span_len)
    )
    own_weight = (own_exp / total).astype(BF16).astype(F32).reshape(row_count, local_kv, group)
    mixed = jnp.einsum("bkgl,bkdl->bkgd", past_weight, value_heads, preferred_element_type=F32)
    own_value = new_values.astype(F32).reshape(row_count, local_kv, 1, HEAD_DIM)
    mixed = mixed + own_weight[:, :, :, None] * own_value
    heads_out = mixed.astype(BF16).reshape(row_count, query_cols)
    layer_out = experts(
        nz,
        ny,
        heads_out,
        tokens,
        norm_gain_mix[None, :],
        norm_gain_ffn[None, :],
        routes,
        route_weights,
        w_out,
        expert_gate,
        expert_up,
        expert_down,
    )
    return (layer_out, new_keys, new_values, new_log_gate)


def solution(mesh):
    placed = (
        P("ep", None),
        P(),
        P("ep", "tp"),
        P("ep", "tp"),
        P("ep", "tp"),
        P(None, "tp"),
        P("tp"),
        P("ep", "tp", None),
        P("ep", "tp", None),
        P("ep", "tp", None),
        P("ep"),
        P("tp", None),
        P(),
        P(),
        P(None, ("ep", "tp")),
        P(None, ("ep", "tp")),
        P(("ep", "tp"), None),
        P("ep", None),
        P("ep", None),
    )
    nz = mesh.shape["ep"] // (NX * NC)
    return jax.shard_map(
        functools.partial(body, nz, mesh.shape["tp"]),
        mesh=mesh,
        in_specs=placed,
        out_specs=(P("ep", "tp"), P("ep", "tp"), P("ep", "tp"), P("ep", "tp")),
        check_vma=False,
    )
```

```python
import functools

import jax
import jax.numpy as jnp
from jax import lax
from jax.experimental import pallas as pl
from jax.experimental.pallas import tpu as pltpu
from jax.sharding import PartitionSpec as P

HEAD_DIM = 64
NX = 4
NC = 2
FLAT = NX * NC
SLOTS = 8
TOGETHER = 8
EPSILON = 1e-06
MASKED = -1e30
MESH = pl.DeviceIdType.MESH
F32 = jnp.float32
BF16 = jnp.bfloat16
EXACT = lax.Precision.HIGHEST
ACROSS = (((1,), (1,)), ((), ()))


def rms_scaled(field, gain_vector):
    return (
        field * lax.rsqrt(jnp.mean(field * field, axis=-1, keepdims=True) + EPSILON) * gain_vector
    )


def log_sigmoid(v):
    return jnp.minimum(v, 0.0) - jnp.log1p(jnp.exp(-jnp.abs(v)))


def dot(a, b):
    return jnp.dot(a, b, preferred_element_type=F32)


def dot_across(a, b, precision=None):
    return lax.dot_general(a, b, ACROSS, precision=precision, preferred_element_type=F32)


def iota(shape, dim):
    return lax.broadcasted_iota(jnp.int32, shape, dim)


def ones_where(mask):
    return jnp.where(mask, 1.0, 0.0).astype(F32)


def remote(src, dst, send, recv, ep, y):
    return pltpu.make_async_remote_copy(
        src_ref=src, dst_ref=dst, send_sem=send, recv_sem=recv, device_id=(ep, y), device_id_type=MESH
    )


def slotted(first, second, expert_of, slot_of, axis):
    in_first, in_second = first == expert_of, second == expert_of
    member = ones_where(in_first | in_second)
    rows = member.shape[axis]
    if axis == 0:
        before = ones_where(iota((rows, rows), 1) < iota((rows, rows), 0)).astype(BF16)
        earlier = dot(before, member.astype(BF16))
    else:
        before = ones_where(iota((rows, rows), 0) < iota((rows, rows), 1)).astype(BF16)
        earlier = dot(member.astype(BF16), before)
    return jnp.where(earlier == slot_of.astype(F32), member, 0.0), in_first, in_second


def nearest_first(n):
    return [(p + 1) // 2 if p % 2 else (n - p // 2) % n for p in range(n)]


def layer_kernel(nz, ny, *refs):
    (tokens, gain_attn, w_query, w_key, w_value, w_forget, forget_bias, lengths) = refs[:8]
    (gain_mix, gain_ffn, routes_across, weights_across) = refs[8:12]
    (keys, values, logcum, w_out, gate, up, down) = refs[12:19]
    (out, new_keys, new_values, new_log_gate) = refs[19:23]
    (keys_v, values_v, logcum_v, wo_v, gate_v, up_v, down_v) = refs[23:30]
    (w_own, w_in, normed, t_in, sums, p_out, p_in) = refs[30:37]
    (query_s, own_value_s, columns_s, heads_s) = refs[37:41]
    (mix_out, mix_in, mixed_res, packed, z_in, x_in, share_out, share_in, back_out, back_in) = refs[41:51]
    (load_sem, w_sem, t_sem, p_sem, pair_sem, y_sem, z_sem, x_sem, s_sem, b_sem) = refs[51:]

    ep, y = lax.axis_index("ep"), lax.axis_index("tp")
    z = lax.div(ep, FLAT)
    at = lax.rem(ep, FLAT)
    x, c = lax.div(at, NC), lax.rem(at, NC)
    rows, width = tokens.shape
    part = width // ny
    query_cols = w_query.shape[1]
    heads = query_cols // HEAD_DIM
    stacked = rows * heads
    span = keys.shape[2]

    def chip(dz, dx):
        return lax.rem(z + dz, nz) * FLAT + lax.rem(x + dx, NX) * NC + c

    def row_peer(d):
        return z * FLAT + lax.rem(at + d, FLAT)

    def y_peer(d):
        return lax.rem(y + d, ny)

    partner = ep + 1 - 2 * c
    barrier = pltpu.get_barrier_semaphore()

    def signal(ep_to, y_to):
        pl.semaphore_signal(barrier, inc=1, device_id=(ep_to, y_to), device_id_type=MESH)

    for dz in range(nz):
        for dx in range(NX):
            if dz or dx:
                signal(chip(dz, dx), y)
    for dx in range(NX):
        signal(z * FLAT + lax.rem(x + dx, NX) * NC + 1 - c, y)
    for d in range(1, ny):
        signal(ep, y_peer(d))

    loads = [
        pltpu.make_async_copy(src, dst, load_sem.at[i])
        for i, (src, dst) in enumerate(
            (
                (keys, keys_v),
                (logcum, logcum_v),
                (values, values_v),
                (w_out, wo_v),
                (gate, gate_v.at[0]),
                (up, up_v.at[0]),
                (down, down_v.at[0]),
            )
        )
    ]
    for load in loads:
        load.start()

    w_own[:, :query_cols] = w_query[...]
    w_own[:, query_cols : query_cols + HEAD_DIM] = w_key[...]
    w_own[:, query_cols + HEAD_DIM :] = w_value[...]
    scaled = rms_scaled(tokens[...].astype(F32), gain_attn[...]).astype(BF16)
    slab = width // nz
    for k in range(nz):
        normed[k] = scaled[:, k * slab : (k + 1) * slab]
    pl.semaphore_wait(barrier, nz * NX - 1 + NX + ny - 1)

    near_first = nearest_first(nz)
    far_first = near_first[:0:-1]
    w_copies = [
        remote(w_own, w_in.at[at], w_sem.at[0, d], w_sem.at[1, d], row_peer(d), y)
        for d in range(1, FLAT)
    ]
    t_copies = [
        remote(normed.at[lax.rem(z + d, nz)], t_in.at[d], t_sem.at[0, d], t_sem.at[1, d], chip(d, 0), y)
        for d in far_first
    ]
    for copy in t_copies + w_copies:
        copy.start()
    w_in[at] = w_own[...]
    t_in[0] = normed[z]
    log_gate = log_sigmoid(dot_across(scaled, w_forget[...]) + forget_bias[...])
    new_log_gate[...] = log_sigmoid(
        dot_across(w_forget[...], scaled) + jnp.transpose(jnp.broadcast_to(forget_bias[...], (rows, heads)))
    )
    for copy in w_copies + t_copies:
        copy.wait_recv()
    product = dot(
        t_in[...].reshape(nz * rows, slab), w_in[...].reshape(FLAT * w_own.shape[0], w_own.shape[1])
    )
    for d in range(1, nz):
        p_out[d] = product[d * rows : (d + 1) * rows].astype(BF16)
    sums[...] = product[:rows]
    p_copies = [
        remote(p_out.at[d], p_in.at[d], p_sem.at[0, d], p_sem.at[1, d], chip(nz - d, 0), y)
        for d in far_first
    ]
    for copy in p_copies:
        copy.start()
    shape = (nz * 2 * SLOTS, rows)
    lane = iota(shape, 0)
    expert_of = 2 * lax.rem(z + lane // (2 * SLOTS), nz) + (lane // SLOTS) % 2
    picking, _, _ = slotted(routes_across[0:1, :], routes_across[1:2, :], expert_of, lane % SLOTS, 1)
    picking = picking.astype(BF16)
    unit = ones_where(iota((rows, rows), 0) == iota((rows, rows), 1))
    routes = dot_across(unit, routes_across[...].astype(F32)).astype(jnp.int32)
    weights = dot_across(unit, weights_across[...], EXACT)
    shape = (rows, nz * NX * SLOTS)
    lane = iota(shape, 1)
    place = lane // (NX * SLOTS)
    dz_of = jnp.where(place % 2 == 1, (place + 1) // 2, nz - place // 2)
    expert_of = 2 * lax.rem(z + dz_of, nz) + lax.rem(x + (lane // SLOTS) % NX, NX) // 2
    weighing, in_first, in_second = slotted(routes[:, 0:1], routes[:, 1:2], expert_of, lane % SLOTS, 0)
    weighing = weighing * (
        jnp.where(in_first, weights[:, 0:1], 0.0) + jnp.where(in_second, weights[:, 1:2], 0.0)
    )
    coarse = weighing.astype(BF16)
    fine = (weighing - coarse.astype(F32)).astype(BF16)
    repeat = ones_where(iota((stacked, rows), 0) // heads == iota((stacked, rows), 1))
    gate_of = jnp.dot(repeat, log_gate, precision=EXACT, preferred_element_type=F32)
    own_head = iota((stacked, heads), 1) == iota((stacked, heads), 0) % heads
    gate_of = jnp.sum(jnp.where(own_head, gate_of, 0.0), axis=1, keepdims=True)
    repeat = repeat.astype(BF16)
    fold = ones_where(iota((query_cols, HEAD_DIM), 0) % HEAD_DIM == iota((query_cols, HEAD_DIM), 1))
    fold = fold.astype(BF16)
    own_part = iota((stacked, query_cols), 1) // HEAD_DIM == iota((stacked, query_cols), 0) % heads
    total = sums[...]
    for copy in p_copies[::-1]:
        copy.wait_recv()
    for d in range(1, nz):
        total = total + p_in[d].astype(F32)
    projected = total.astype(BF16)
    new_key = projected[:, query_cols : query_cols + HEAD_DIM]
    new_value = projected[:, query_cols + HEAD_DIM :]
    new_keys[...] = new_key
    new_values[...] = new_value

    pair_copies = [
        remote(src, dst.at[1], pair_sem.at[0, i], pair_sem.at[1, i], partner, y)
        for i, (src, dst) in enumerate(((gate, gate_v), (up, up_v), (down, down_v)))
    ]
    for copy in pair_copies:
        copy.start()
    spread = jnp.where(own_part, dot(repeat, projected[:, :query_cols]), 0.0).astype(BF16)
    query_of = dot(spread, fold) * HEAD_DIM ** (-0.5)
    query_s[...] = query_of
    columns_s[:, 0:1] = jnp.sum(query_of * dot(repeat, new_key), axis=1, keepdims=True)
    columns_s[:, 1:2] = gate_of
    own_value_s[...] = dot(repeat, new_value)
    for load in loads[:3]:
        load.wait()

    def attend(step, carry):
        group = []
        for j in range(TOGETHER):
            b = step * TOGETHER + j
            at_rows = pl.ds(pl.multiple_of(b * heads, heads), heads)
            score = dot(query_s[at_rows, :].astype(BF16), keys_v[b])
            group.append((b, at_rows, score))
        for j, (b, at_rows, score) in enumerate(group):
            cum = logcum_v[b]
            length = lengths[b]
            position = iota((heads, span), 1)
            last = jnp.sum(jnp.where(position == length - 1, cum, 0.0), axis=1, keepdims=True)
            own = columns_s[at_rows, 0:1]
            shift = (last + columns_s[at_rows, 1:2]) - cum
            past = jnp.where(position < length, score + shift, MASKED)
            peak = jnp.maximum(jnp.max(past, axis=1, keepdims=True), own)
            past = jnp.exp(past - peak)
            own = jnp.exp(own - peak)
            group[j] = (b, at_rows, past, own, jnp.sum(past, axis=1, keepdims=True) + own)
        for b, at_rows, past, own, norm in group:
            mixed = dot_across(past.astype(BF16), values_v[b]) + own * own_value_s[at_rows, :]
            heads_s[at_rows, :] = mixed / norm
        return carry

    lax.fori_loop(0, rows // TOGETHER, attend, 0)
    spread = jnp.where(own_part, dot_across(heads_s[...].astype(BF16), fold), 0.0).astype(BF16)
    gather = ones_where(iota((rows, stacked), 1) // heads == iota((rows, stacked), 0)).astype(BF16)
    heads_out = dot(gather, spread).astype(BF16)
    loads[3].wait()
    mix_out[...] = dot(heads_out, wo_v[...]).astype(BF16)

    y_copies = [
        remote(mix_out, mix_in.at[d], y_sem.at[0, d], y_sem.at[1, d], ep, y_peer(d)) for d in range(1, ny)
    ]
    for copy in y_copies:
        copy.start()
    for copy in w_copies + t_copies + p_copies:
        copy.wait_send()
    for load in loads[4:]:
        load.wait()
    mix = mix_out[...].astype(F32)
    for i, copy in enumerate(y_copies):
        copy.wait_recv()
        mix = mix + mix_in[i + 1].astype(F32)
    mixed = tokens[...].astype(F32) + rms_scaled(mix, gain_mix[...])
    for k in range(ny):
        mixed_res[k] = mixed[:, k * part : (k + 1) * part]
    ffn_in = rms_scaled(mixed, gain_ffn[...]).astype(BF16)
    packed[...] = dot(picking, ffn_in).astype(BF16).reshape(nz, 2, SLOTS, width)

    z_copies = [None] + [
        remote(packed.at[d], z_in.at[p], z_sem.at[0, p], z_sem.at[1, p], chip(d, 0), y)
        for p, d in enumerate(near_first)
        if p
    ]
    for copy in z_copies[1:]:
        copy.start()
    z_in[0] = packed[0]
    x_copies, s_copies, b_copies = {}, {}, []
    chunks = [(0, 3), (3, 5), (5, 7), (7, 8)] if nz == 8 else [(p, p + 1) for p in range(nz)]

    def forward(chunk):
        for p in range(*chunk):
            if p:
                z_copies[p].wait_recv()
            for dx in range(1, NX):
                half = lax.rem(x + dx, NX) // 2
                x_copies[p, dx] = remote(
                    z_in.at[p, half], x_in.at[p, dx], x_sem.at[0, p, dx], x_sem.at[1, p, dx], chip(0, dx), y
                )
                x_copies[p, dx].start()
            x_in[p, 0] = z_in[p, x // 2]

    def multiply(chunk):
        lo, hi = chunk
        for p in range(lo, hi):
            for dx in range(1, NX):
                x_copies[p, dx].wait_recv()
        if lo == 0:
            for copy in pair_copies:
                copy.wait_recv()
        count = (hi - lo) * NX * SLOTS
        first = lo * NX * SLOTS
        arrived = x_in[lo:hi].reshape(count, width)
        hidden = []
        for k in range(NC):
            gate_part = dot(arrived, gate_v[k])
            up_part = dot(arrived, up_v[k])
            hidden.append((gate_part / (1.0 + jnp.exp(-gate_part)) * up_part).astype(BF16))
        for j in range(ny):
            cols = slice(j * part, (j + 1) * part)
            share = dot(hidden[0], down_v[0, :, cols]) + dot(hidden[1], down_v[1, :, cols])
            share_out[j, first : first + count] = share.astype(BF16)
        for d in range(1, ny):
            s_copies[lo, d] = remote(
                share_out.at[y_peer(d), pl.ds(first, count)],
                share_in.at[d, pl.ds(first, count)],
                s_sem.at[0, lo, d],
                s_sem.at[1, lo, d],
                ep,
                y_peer(d),
            )
            s_copies[lo, d].start()

    def give_back(chunk):
        lo, hi = chunk
        count = (hi - lo) * NX * SLOTS
        here = pl.ds(lo * NX * SLOTS, count)
        total = share_out[y, here].astype(F32)
        for d in range(1, ny):
            s_copies[lo, d].wait_recv()
            total = total + share_in[d, here].astype(F32)
        back_out[lo:hi] = total.astype(BF16).reshape(hi - lo, NX, SLOTS, part)
        for p in range(lo, hi):
            for dx in range(NX):
                if p or dx:
                    copy = remote(
                        back_out.at[p, dx],
                        back_in.at[p, dx],
                        b_sem.at[0, p, dx],
                        b_sem.at[1, p, dx],
                        chip(nz - near_first[p], NX - dx),
                        y,
                    )
                    copy.start()
                    b_copies.append(copy)
                else:
                    back_in[0, 0] = back_out[0, 0]

    forward(chunks[0])
    for i, chunk in enumerate(chunks):
        if i + 1 < len(chunks):
            forward(chunks[i + 1])
        multiply(chunk)
        if i:
            give_back(chunks[i - 1])
    give_back(chunks[-1])
    for copy in y_copies + pair_copies + z_copies[1:] + list(x_copies.values()) + list(s_copies.values()):
        copy.wait_send()
    for copy in b_copies:
        copy.wait_recv()
    returned = back_in[...].reshape(nz * NX * SLOTS, part)
    out[...] = (mixed_res[y] + (dot(coarse, returned) + dot(fine, returned))).astype(BF16)
    for copy in b_copies:
        copy.wait_send()


def body(
    nz,
    ny,
    tokens,
    norm_gain_attn,
    w_query,
    w_key,
    w_value,
    w_forget,
    forget_bias,
    cache_keys,
    cache_values,
    cache_logcum,
    lengths,
    w_out,
    norm_gain_mix,
    norm_gain_ffn,
    expert_gate,
    expert_up,
    expert_down,
    routes,
    route_weights,
):
    rows, width = tokens.shape
    part = width // ny
    query_cols = w_query.shape[1]
    cols = query_cols + w_key.shape[1] + w_value.shape[1]
    heads = query_cols // HEAD_DIM
    hidden = expert_gate.shape[1]
    depth = w_query.shape[0]
    stacked = rows * heads
    lanes = nz * NX * SLOTS
    vmem = pl.BlockSpec(memory_space=pltpu.VMEM)
    kept = pl.BlockSpec(memory_space=pl.ANY)
    smem = pl.BlockSpec(memory_space=pltpu.SMEM)

    def dma(*shape):
        return pltpu.SemaphoreType.DMA((2, *shape))

    layer_out, new_keys, new_values, new_log_gate = pl.pallas_call(
        functools.partial(layer_kernel, nz, ny),
        out_shape=(
            jax.ShapeDtypeStruct((rows, part), BF16),
            jax.ShapeDtypeStruct((rows, HEAD_DIM), BF16),
            jax.ShapeDtypeStruct((rows, HEAD_DIM), BF16),
            jax.ShapeDtypeStruct((heads, rows), F32),
        ),
        in_specs=[vmem] * 7 + [smem] + [vmem] * 4 + [kept] * 7,
        out_specs=(vmem,) * 4,
        scratch_shapes=[
            pltpu.VMEM(cache_keys.shape, BF16),
            pltpu.VMEM(cache_values.shape, BF16),
            pltpu.VMEM(cache_logcum.shape, F32),
            pltpu.VMEM(w_out.shape, BF16),
            pltpu.VMEM((NC, width, hidden), BF16),
            pltpu.VMEM((NC, width, hidden), BF16),
            pltpu.VMEM((NC, hidden, width), BF16),
            pltpu.VMEM((depth, cols), BF16),
            pltpu.VMEM((FLAT, depth, cols), BF16),
            pltpu.VMEM((nz, rows, width // nz), BF16),
            pltpu.VMEM((nz, rows, width // nz), BF16),
            pltpu.VMEM((rows, cols), F32),
            pltpu.VMEM((nz, rows, cols), BF16),
            pltpu.VMEM((nz, rows, cols), BF16),
            pltpu.VMEM((stacked, HEAD_DIM), F32),
            pltpu.VMEM((stacked, HEAD_DIM), F32),
            pltpu.VMEM((stacked, 2), F32),
            pltpu.VMEM((stacked, HEAD_DIM), F32),
            pltpu.VMEM((rows, width), BF16),
            pltpu.VMEM((ny, rows, width), BF16),
            pltpu.VMEM((ny, rows, part), F32),
            pltpu.VMEM((nz, 2, SLOTS, width), BF16),
            pltpu.VMEM((nz, 2, SLOTS, width), BF16),
            pltpu.VMEM((nz, NX, SLOTS, width), BF16),
            pltpu.VMEM((ny, lanes, part), BF16),
            pltpu.VMEM((ny, lanes, part), BF16),
            pltpu.VMEM((nz, NX, SLOTS, part), BF16),
            pltpu.VMEM((nz, NX, SLOTS, part), BF16),
            pltpu.SemaphoreType.DMA((7,)),
            dma(FLAT),
            dma(nz),
            dma(nz),
            dma(3),
            dma(ny),
            dma(nz),
            dma(nz, NX),
            dma(nz, ny),
            dma(nz, NX),
        ],
        compiler_params=pltpu.CompilerParams(collective_id=0, has_side_effects=True),
        name="layer",
    )(
        tokens,
        norm_gain_attn[None, :],
        w_query,
        w_key,
        w_value,
        w_forget.T,
        forget_bias[None, :],
        lengths,
        norm_gain_mix[None, :],
        norm_gain_ffn[None, :],
        routes.T,
        route_weights.T,
        cache_keys,
        cache_values,
        cache_logcum,
        w_out,
        expert_gate,
        expert_up,
        expert_down,
    )
    return layer_out, new_keys, new_values, new_log_gate.T


def solution(mesh):
    placed = (
        P("ep", None),
        P(),
        P("ep", "tp"),
        P("ep", "tp"),
        P("ep", "tp"),
        P(None, "tp"),
        P("tp"),
        P("ep", "tp", None),
        P("ep", "tp", None),
        P("ep", "tp", None),
        P("ep"),
        P("tp", None),
        P(),
        P(),
        P(None, ("ep", "tp")),
        P(None, ("ep", "tp")),
        P(("ep", "tp"), None),
        P("ep", None),
        P("ep", None),
    )
    nz = mesh.shape["ep"] // FLAT
    return jax.shard_map(
        functools.partial(body, nz, mesh.shape["tp"]),
        mesh=mesh,
        in_specs=placed,
        out_specs=(P("ep", "tp"), P("ep", "tp"), P("ep", "tp"), P("ep", "tp")),
        check_vma=False,
    )
```

```python
import functools

import jax
import jax.numpy as jnp
from jax import lax
from jax.experimental import pallas as pl
from jax.experimental.pallas import tpu as pltpu
from jax.sharding import PartitionSpec as P

HEAD_DIM = 64
NX = 4
NC = 2
FLAT = NX * NC
SLOTS = 8
TOGETHER = 8
HALVES = 2
EPSILON = 1e-06
MASKED = -1e30
MESH = pl.DeviceIdType.MESH
F32 = jnp.float32
BF16 = jnp.bfloat16
EXACT = lax.Precision.HIGHEST
ACROSS = (((1,), (1,)), ((), ()))


def rms_scaled(field, gain_vector):
    return (
        field * lax.rsqrt(jnp.mean(field * field, axis=-1, keepdims=True) + EPSILON) * gain_vector
    )


def log_sigmoid(v):
    return jnp.minimum(v, 0.0) - jnp.log1p(jnp.exp(-jnp.abs(v)))


def dot(a, b):
    return jnp.dot(a, b, preferred_element_type=F32)


def dot_across(a, b, precision=None):
    return lax.dot_general(a, b, ACROSS, precision=precision, preferred_element_type=F32)


def iota(shape, dim):
    return lax.broadcasted_iota(jnp.int32, shape, dim)


def ones_where(mask):
    return jnp.where(mask, 1.0, 0.0).astype(F32)


def remote(src, dst, send, recv, ep, y):
    return pltpu.make_async_remote_copy(
        src_ref=src, dst_ref=dst, send_sem=send, recv_sem=recv, device_id=(ep, y), device_id_type=MESH
    )


def slotted(first, second, expert_of, slot_of, axis):
    in_first, in_second = first == expert_of, second == expert_of
    member = ones_where(in_first | in_second)
    rows = member.shape[axis]
    if axis == 0:
        before = ones_where(iota((rows, rows), 1) < iota((rows, rows), 0)).astype(BF16)
        earlier = dot(before, member.astype(BF16))
    else:
        before = ones_where(iota((rows, rows), 0) < iota((rows, rows), 1)).astype(BF16)
        earlier = dot(member.astype(BF16), before)
    return jnp.where(earlier == slot_of.astype(F32), member, 0.0), in_first, in_second


def nearest_first(n):
    return [(p + 1) // 2 if p % 2 else (n - p // 2) % n for p in range(n)]


def layer_kernel(nz, ny, *refs):
    (tokens, gain_attn, w_query, w_key, w_value, w_forget, forget_bias, lengths) = refs[:8]
    (gain_mix, gain_ffn, routes_across, weights_across) = refs[8:12]
    (keys, values, logcum, w_out, gate, up, down) = refs[12:19]
    (out, new_keys, new_values, new_log_gate) = refs[19:23]
    (keys_v, values_v, logcum_v, wo_v, gate_v, up_v, down_v) = refs[23:30]
    (w_own, w_in, normed, t_in, sums, p_out, p_in) = refs[30:37]
    (query_s, own_value_s, columns_s, heads_s) = refs[37:41]
    (mix_out, mix_in, mixed_res, packed, z_in, x_in, share_out, share_in, back_out, back_in) = refs[41:51]
    (load_sem, w_sem, t_sem, p_sem, pair_sem, y_sem, z_sem, x_sem, s_sem, b_sem) = refs[51:]

    ep, y = lax.axis_index("ep"), lax.axis_index("tp")
    z = lax.div(ep, FLAT)
    at = lax.rem(ep, FLAT)
    x, c = lax.div(at, NC), lax.rem(at, NC)
    rows, width = tokens.shape
    part = width // ny
    query_cols = w_query.shape[1]
    heads = query_cols // HEAD_DIM
    stacked = rows * heads
    span = keys.shape[2]

    def chip(dz, dx):
        return lax.rem(z + dz, nz) * FLAT + lax.rem(x + dx, NX) * NC + c

    def row_peer(d):
        return z * FLAT + lax.rem(at + d, FLAT)

    def y_peer(d):
        return lax.rem(y + d, ny)

    partner = ep + 1 - 2 * c
    barrier = pltpu.get_barrier_semaphore()

    def signal(ep_to, y_to):
        pl.semaphore_signal(barrier, inc=1, device_id=(ep_to, y_to), device_id_type=MESH)

    for d in range(1, nz):
        signal(chip(d, 0), y)
    for d in range(1, FLAT):
        signal(row_peer(d), y)
    for d in range(1, ny):
        signal(ep, y_peer(d))

    loads = [
        pltpu.make_async_copy(src, dst, load_sem.at[i])
        for i, (src, dst) in enumerate(
            (
                (keys, keys_v),
                (logcum, logcum_v),
                (values, values_v),
                (w_out, wo_v),
                (gate, gate_v.at[0]),
                (up, up_v.at[0]),
                (down, down_v.at[0]),
            )
        )
    ]
    for load in loads:
        load.start()

    w_own[:, :query_cols] = w_query[...]
    w_own[:, query_cols : query_cols + HEAD_DIM] = w_key[...]
    w_own[:, query_cols + HEAD_DIM :] = w_value[...]
    scaled = rms_scaled(tokens[...].astype(F32), gain_attn[...]).astype(BF16)
    slab = width // nz
    for k in range(nz):
        normed[k] = scaled[:, k * slab : (k + 1) * slab]
    pl.semaphore_wait(barrier, nz - 1 + FLAT - 1 + ny - 1)

    near_first = nearest_first(nz)
    far_first = near_first[:0:-1]
    w_copies = [
        remote(w_own, w_in.at[at], w_sem.at[0, d], w_sem.at[1, d], row_peer(d), y)
        for d in range(1, FLAT)
    ]
    t_copies = [
        remote(normed.at[lax.rem(z + d, nz)], t_in.at[d], t_sem.at[0, d], t_sem.at[1, d], chip(d, 0), y)
        for d in far_first
    ]
    for copy in t_copies + w_copies:
        copy.start()
    w_in[at] = w_own[...]
    t_in[0] = normed[z]
    log_gate = log_sigmoid(dot_across(scaled, w_forget[...]) + forget_bias[...])
    new_log_gate[...] = log_sigmoid(
        dot_across(w_forget[...], scaled) + jnp.transpose(jnp.broadcast_to(forget_bias[...], (rows, heads)))
    )
    for copy in w_copies + t_copies:
        copy.wait_recv()
    product = dot(
        t_in[...].reshape(nz * rows, slab), w_in[...].reshape(FLAT * w_own.shape[0], w_own.shape[1])
    )
    for d in range(1, nz):
        p_out[d] = product[d * rows : (d + 1) * rows].astype(BF16)
    sums[...] = product[:rows]
    p_copies = [
        remote(p_out.at[d], p_in.at[d], p_sem.at[0, d], p_sem.at[1, d], chip(nz - d, 0), y)
        for d in far_first
    ]
    for copy in p_copies:
        copy.start()
    shape = (nz * 2 * SLOTS, rows)
    lane = iota(shape, 0)
    expert_of = 2 * lax.rem(z + lane // (2 * SLOTS), nz) + (lane // SLOTS) % 2
    picking, _, _ = slotted(routes_across[0:1, :], routes_across[1:2, :], expert_of, lane % SLOTS, 1)
    picking = picking.astype(BF16)
    unit = ones_where(iota((rows, rows), 0) == iota((rows, rows), 1))
    routes = dot_across(unit, routes_across[...].astype(F32)).astype(jnp.int32)
    weights = dot_across(unit, weights_across[...], EXACT)
    shape = (rows, nz * NX * SLOTS)
    lane = iota(shape, 1)
    place = lane // (NX * SLOTS)
    dz_of = jnp.where(place % 2 == 1, (place + 1) // 2, nz - place // 2)
    expert_of = 2 * lax.rem(z + dz_of, nz) + lax.rem(x + (lane // SLOTS) % NX, NX) // 2
    weighing, in_first, in_second = slotted(routes[:, 0:1], routes[:, 1:2], expert_of, lane % SLOTS, 0)
    weighing = weighing * (
        jnp.where(in_first, weights[:, 0:1], 0.0) + jnp.where(in_second, weights[:, 1:2], 0.0)
    )
    coarse = weighing.astype(BF16)
    fine = (weighing - coarse.astype(F32)).astype(BF16)
    repeat = ones_where(iota((stacked, rows), 0) // heads == iota((stacked, rows), 1))
    gate_of = jnp.dot(repeat, log_gate, precision=EXACT, preferred_element_type=F32)
    own_head = iota((stacked, heads), 1) == iota((stacked, heads), 0) % heads
    gate_of = jnp.sum(jnp.where(own_head, gate_of, 0.0), axis=1, keepdims=True)
    repeat = repeat.astype(BF16)
    fold = ones_where(iota((query_cols, HEAD_DIM), 0) % HEAD_DIM == iota((query_cols, HEAD_DIM), 1))
    fold = fold.astype(BF16)
    own_part = iota((stacked, query_cols), 1) // HEAD_DIM == iota((stacked, query_cols), 0) % heads
    total = sums[...]
    for copy in p_copies[::-1]:
        copy.wait_recv()
    for d in range(1, nz):
        total = total + p_in[d].astype(F32)
    projected = total.astype(BF16)
    new_key = projected[:, query_cols : query_cols + HEAD_DIM]
    new_value = projected[:, query_cols + HEAD_DIM :]
    new_keys[...] = new_key
    new_values[...] = new_value

    pair_copies = [
        remote(src, dst.at[1], pair_sem.at[0, i], pair_sem.at[1, i], partner, y)
        for i, (src, dst) in enumerate(((gate, gate_v), (up, up_v), (down, down_v)))
    ]
    for copy in pair_copies:
        copy.start()
    spread = jnp.where(own_part, dot(repeat, projected[:, :query_cols]), 0.0).astype(BF16)
    query_of = dot(spread, fold) * HEAD_DIM ** (-0.5)
    query_s[...] = query_of
    columns_s[:, 0:1] = jnp.sum(query_of * dot(repeat, new_key), axis=1, keepdims=True)
    columns_s[:, 1:2] = gate_of
    own_value_s[...] = dot(repeat, new_value)
    for load in loads[:3]:
        load.wait()

    def attend(step, carry):
        group = []
        for j in range(TOGETHER):
            b = step * TOGETHER + j
            at_rows = pl.ds(pl.multiple_of(b * heads, heads), heads)
            score = dot(query_s[at_rows, :].astype(BF16), keys_v[b])
            group.append((b, at_rows, score))
        for j, (b, at_rows, score) in enumerate(group):
            cum = logcum_v[b]
            length = lengths[b]
            position = iota((heads, span), 1)
            last = jnp.sum(jnp.where(position == length - 1, cum, 0.0), axis=1, keepdims=True)
            own = columns_s[at_rows, 0:1]
            shift = (last + columns_s[at_rows, 1:2]) - cum
            past = jnp.where(position < length, score + shift, MASKED)
            peak = jnp.maximum(jnp.max(past, axis=1, keepdims=True), own)
            past = jnp.exp(past - peak)
            own = jnp.exp(own - peak)
            group[j] = (b, at_rows, past, own, jnp.sum(past, axis=1, keepdims=True) + own)
        for b, at_rows, past, own, norm in group:
            mixed = dot_across(past.astype(BF16), values_v[b]) + own * own_value_s[at_rows, :]
            heads_s[at_rows, :] = mixed / norm
        return carry

    y_copies = []
    count = rows // HALVES
    gather = ones_where(iota((count, count * heads), 1) // heads == iota((count, count * heads), 0)).astype(BF16)
    for half in range(HALVES):
        steps = count // TOGETHER
        lax.fori_loop(half * steps, (half + 1) * steps, attend, 0)
        lo = half * count * heads
        mixed = heads_s[lo : lo + count * heads, :].astype(BF16)
        spread = jnp.where(own_part[: count * heads], dot_across(mixed, fold), 0.0).astype(BF16)
        heads_out = dot(gather, spread).astype(BF16)
        if half == 0:
            loads[3].wait()
        mix_out[half] = dot(heads_out, wo_v[...]).astype(BF16)
        for d in range(1, ny):
            copy = remote(
                mix_out.at[half],
                mix_in.at[d, half],
                y_sem.at[0, d, half],
                y_sem.at[1, d, half],
                ep,
                y_peer(d),
            )
            copy.start()
            y_copies.append(copy)
    for copy in w_copies + t_copies + p_copies:
        copy.wait_send()
    for load in loads[4:]:
        load.wait()
    mix = mix_out[...].reshape(rows, width).astype(F32)
    for copy in y_copies:
        copy.wait_recv()
    for d in range(1, ny):
        mix = mix + mix_in[d].reshape(rows, width).astype(F32)
    mixed = tokens[...].astype(F32) + rms_scaled(mix, gain_mix[...])
    for k in range(ny):
        mixed_res[k] = mixed[:, k * part : (k + 1) * part]
    ffn_in = rms_scaled(mixed, gain_ffn[...]).astype(BF16)
    packed[...] = dot(picking, ffn_in).astype(BF16).reshape(nz, 2, SLOTS, width)

    z_copies = [None] + [
        remote(packed.at[d], z_in.at[p], z_sem.at[0, p], z_sem.at[1, p], chip(d, 0), y)
        for p, d in enumerate(near_first)
        if p
    ]
    for copy in z_copies[1:]:
        copy.start()
    z_in[0] = packed[0]
    x_copies, s_copies, b_copies = {}, {}, []
    chunks = [(0, 3), (3, 5), (5, 7), (7, 8)] if nz == 8 else [(p, p + 1) for p in range(nz)]

    def forward(chunk):
        for p in range(*chunk):
            if p:
                z_copies[p].wait_recv()
            for dx in range(1, NX):
                half = lax.rem(x + dx, NX) // 2
                x_copies[p, dx] = remote(
                    z_in.at[p, half], x_in.at[p, dx], x_sem.at[0, p, dx], x_sem.at[1, p, dx], chip(0, dx), y
                )
                x_copies[p, dx].start()
            x_in[p, 0] = z_in[p, x // 2]

    def multiply(chunk):
        lo, hi = chunk
        for p in range(lo, hi):
            for dx in range(1, NX):
                x_copies[p, dx].wait_recv()
        if lo == 0:
            for copy in pair_copies:
                copy.wait_recv()
        count = (hi - lo) * NX * SLOTS
        first = lo * NX * SLOTS
        arrived = x_in[lo:hi].reshape(count, width)
        hidden = []
        for k in range(NC):
            gate_part = dot(arrived, gate_v[k])
            up_part = dot(arrived, up_v[k])
            hidden.append((gate_part / (1.0 + jnp.exp(-gate_part)) * up_part).astype(BF16))
        for j in range(ny):
            cols = slice(j * part, (j + 1) * part)
            share = dot(hidden[0], down_v[0, :, cols]) + dot(hidden[1], down_v[1, :, cols])
            share_out[j, first : first + count] = share.astype(BF16)
        for d in range(1, ny):
            s_copies[lo, d] = remote(
                share_out.at[y_peer(d), pl.ds(first, count)],
                share_in.at[d, pl.ds(first, count)],
                s_sem.at[0, lo, d],
                s_sem.at[1, lo, d],
                ep,
                y_peer(d),
            )
            s_copies[lo, d].start()

    def give_back(chunk):
        lo, hi = chunk
        count = (hi - lo) * NX * SLOTS
        here = pl.ds(lo * NX * SLOTS, count)
        total = share_out[y, here].astype(F32)
        for d in range(1, ny):
            s_copies[lo, d].wait_recv()
            total = total + share_in[d, here].astype(F32)
        back_out[lo:hi] = total.astype(BF16).reshape(hi - lo, NX, SLOTS, part)
        for p in range(lo, hi):
            for dx in range(NX):
                if p or dx:
                    copy = remote(
                        back_out.at[p, dx],
                        back_in.at[p, dx],
                        b_sem.at[0, p, dx],
                        b_sem.at[1, p, dx],
                        chip(nz - near_first[p], NX - dx),
                        y,
                    )
                    copy.start()
                    b_copies.append(copy)
                else:
                    back_in[0, 0] = back_out[0, 0]

    forward(chunks[0])
    for i, chunk in enumerate(chunks):
        if i + 1 < len(chunks):
            forward(chunks[i + 1])
        multiply(chunk)
        if i:
            give_back(chunks[i - 1])
    give_back(chunks[-1])
    for copy in y_copies + pair_copies + z_copies[1:] + list(x_copies.values()) + list(s_copies.values()):
        copy.wait_send()
    for copy in b_copies:
        copy.wait_recv()
    returned = back_in[...].reshape(nz * NX * SLOTS, part)
    out[...] = (mixed_res[y] + (dot(coarse, returned) + dot(fine, returned))).astype(BF16)
    for copy in b_copies:
        copy.wait_send()


def write_kernel(*refs):
    for src, dst in zip(refs[:4], refs[4:]):
        dst[...] = src[...]


def body(
    nz,
    ny,
    tokens,
    norm_gain_attn,
    w_query,
    w_key,
    w_value,
    w_forget,
    forget_bias,
    cache_keys,
    cache_values,
    cache_logcum,
    lengths,
    w_out,
    norm_gain_mix,
    norm_gain_ffn,
    expert_gate,
    expert_up,
    expert_down,
    routes,
    route_weights,
):
    rows, width = tokens.shape
    part = width // ny
    query_cols = w_query.shape[1]
    cols = query_cols + w_key.shape[1] + w_value.shape[1]
    heads = query_cols // HEAD_DIM
    hidden = expert_gate.shape[1]
    depth = w_query.shape[0]
    stacked = rows * heads
    lanes = nz * NX * SLOTS
    vmem = pl.BlockSpec(memory_space=pltpu.VMEM)
    kept = pl.BlockSpec(memory_space=pl.ANY)
    smem = pl.BlockSpec(memory_space=pltpu.SMEM)

    def dma(*shape):
        return pltpu.SemaphoreType.DMA((2, *shape))

    results = pl.pallas_call(
        functools.partial(layer_kernel, nz, ny),
        out_shape=(
            jax.ShapeDtypeStruct((rows, part), BF16),
            jax.ShapeDtypeStruct((rows, HEAD_DIM), BF16),
            jax.ShapeDtypeStruct((rows, HEAD_DIM), BF16),
            jax.ShapeDtypeStruct((heads, rows), F32),
        ),
        in_specs=[vmem] * 7 + [smem] + [vmem] * 4 + [kept] * 7,
        out_specs=(vmem,) * 4,
        scratch_shapes=[
            pltpu.VMEM(cache_keys.shape, BF16),
            pltpu.VMEM(cache_values.shape, BF16),
            pltpu.VMEM(cache_logcum.shape, F32),
            pltpu.VMEM(w_out.shape, BF16),
            pltpu.VMEM((NC, width, hidden), BF16),
            pltpu.VMEM((NC, width, hidden), BF16),
            pltpu.VMEM((NC, hidden, width), BF16),
            pltpu.VMEM((depth, cols), BF16),
            pltpu.VMEM((FLAT, depth, cols), BF16),
            pltpu.VMEM((nz, rows, width // nz), BF16),
            pltpu.VMEM((nz, rows, width // nz), BF16),
            pltpu.VMEM((rows, cols), F32),
            pltpu.VMEM((nz, rows, cols), BF16),
            pltpu.VMEM((nz, rows, cols), BF16),
            pltpu.VMEM((stacked, HEAD_DIM), F32),
            pltpu.VMEM((stacked, HEAD_DIM), F32),
            pltpu.VMEM((stacked, 2), F32),
            pltpu.VMEM((stacked, HEAD_DIM), F32),
            pltpu.VMEM((HALVES, rows // HALVES, width), BF16),
            pltpu.VMEM((ny, HALVES, rows // HALVES, width), BF16),
            pltpu.VMEM((ny, rows, part), F32),
            pltpu.VMEM((nz, 2, SLOTS, width), BF16),
            pltpu.VMEM((nz, 2, SLOTS, width), BF16),
            pltpu.VMEM((nz, NX, SLOTS, width), BF16),
            pltpu.VMEM((ny, lanes, part), BF16),
            pltpu.VMEM((ny, lanes, part), BF16),
            pltpu.VMEM((nz, NX, SLOTS, part), BF16),
            pltpu.VMEM((nz, NX, SLOTS, part), BF16),
            pltpu.SemaphoreType.DMA((7,)),
            dma(FLAT),
            dma(nz),
            dma(nz),
            dma(3),
            dma(ny, HALVES),
            dma(nz),
            dma(nz, NX),
            dma(nz, ny),
            dma(nz, NX),
        ],
        compiler_params=pltpu.CompilerParams(collective_id=0, has_side_effects=True),
        name="layer",
    )(
        tokens,
        norm_gain_attn[None, :],
        w_query,
        w_key,
        w_value,
        w_forget.T,
        forget_bias[None, :],
        lengths,
        norm_gain_mix[None, :],
        norm_gain_ffn[None, :],
        routes.T,
        route_weights.T,
        cache_keys,
        cache_values,
        cache_logcum,
        w_out,
        expert_gate,
        expert_up,
        expert_down,
    )
    layer_out, new_keys, new_values, new_log_gate = pl.pallas_call(
        write_kernel,
        out_shape=tuple(jax.ShapeDtypeStruct(a.shape, a.dtype) for a in results),
        in_specs=(vmem,) * 4,
        out_specs=(vmem,) * 4,
        name="write",
    )(*results)
    return layer_out, new_keys, new_values, new_log_gate.T


def solution(mesh):
    placed = (
        P("ep", None),
        P(),
        P("ep", "tp"),
        P("ep", "tp"),
        P("ep", "tp"),
        P(None, "tp"),
        P("tp"),
        P("ep", "tp", None),
        P("ep", "tp", None),
        P("ep", "tp", None),
        P("ep"),
        P("tp", None),
        P(),
        P(),
        P(None, ("ep", "tp")),
        P(None, ("ep", "tp")),
        P(("ep", "tp"), None),
        P("ep", None),
        P("ep", None),
    )
    nz = mesh.shape["ep"] // FLAT
    return jax.shard_map(
        functools.partial(body, nz, mesh.shape["tp"]),
        mesh=mesh,
        in_specs=placed,
        out_specs=(P("ep", "tp"), P("ep", "tp"), P("ep", "tp"), P("ep", "tp")),
        check_vma=False,
    )
```

```python
import functools

import jax
import jax.numpy as jnp
from jax import lax
from jax.experimental import pallas as pl
from jax.experimental.pallas import tpu as pltpu
from jax.sharding import PartitionSpec as P

HEAD_DIM = 64
NX = 4
NC = 2
FLAT = NX * NC
SLOTS = 8
TOGETHER = 8
CHUNKS = ((0, 1), (1, 3), (3, 5), (5, 7), (7, 8))
SCHEDULE = (
    *(("x", 0), ("y", 1), ("y", 2), ("m", 0), ("x", 1), ("x", 2), ("y", 3), ("y", 4), ("x", 3), ("x", 4), ("y", 5)),
    *(("y", 6), ("m", 1), ("x", 5), ("x", 6), ("y", 7), ("r", 0), ("m", 2), ("x", 7), ("r", 1), ("m", 3), ("r", 2)),
    *(("m", 4), ("r", 3), ("r", 4)),
)
EPSILON = 1e-06
MASKED = -1e30
MESH = pl.DeviceIdType.MESH
F32 = jnp.float32
BF16 = jnp.bfloat16
EXACT = lax.Precision.HIGHEST
ACROSS = (((1,), (1,)), ((), ()))


def rms_scaled(field, gain_vector):
    return (
        field * lax.rsqrt(jnp.mean(field * field, axis=-1, keepdims=True) + EPSILON) * gain_vector
    )


def log_sigmoid(v):
    return jnp.minimum(v, 0.0) - jnp.log1p(jnp.exp(-jnp.abs(v)))


def dot(a, b):
    return jnp.dot(a, b, preferred_element_type=F32)


def dot_across(a, b, precision=None):
    return lax.dot_general(a, b, ACROSS, precision=precision, preferred_element_type=F32)


def iota(shape, dim):
    return lax.broadcasted_iota(jnp.int32, shape, dim)


def ones_where(mask):
    return jnp.where(mask, 1.0, 0.0).astype(F32)


def remote(src, dst, send, recv, ep, y):
    return pltpu.make_async_remote_copy(
        src_ref=src, dst_ref=dst, send_sem=send, recv_sem=recv, device_id=(ep, y), device_id_type=MESH
    )


def slotted(first, second, expert_of, slot_of, axis):
    in_first, in_second = first == expert_of, second == expert_of
    member = ones_where(in_first | in_second)
    rows = member.shape[axis]
    if axis == 0:
        before = ones_where(iota((rows, rows), 1) < iota((rows, rows), 0)).astype(BF16)
        earlier = dot(before, member.astype(BF16))
    else:
        before = ones_where(iota((rows, rows), 0) < iota((rows, rows), 1)).astype(BF16)
        earlier = dot(member.astype(BF16), before)
    return jnp.where(earlier == slot_of.astype(F32), member, 0.0), in_first, in_second


def near_order(n):
    return [(p + 1) // 2 if p % 2 else (n - p // 2) % n for p in range(n)]


def of_both(sides, weights, k):
    depth, cols = 2 * weights.shape[3], weights.shape[4]
    return sum(dot(side, weights[k, :, i].reshape(depth, cols)) for i, side in enumerate(sides))


def layer_kernel(nz, ny, *refs):
    small_hbm, (keys, values, logcum, w_out, gate, up, down), lengths = refs[:11], refs[11:18], refs[18]
    results_hbm, small, results_v = refs[19:23], refs[23:34], refs[34:38]
    (tokens, gain_attn, w_query, w_key, w_value, w_forget, forget_bias) = small[:7]
    (gain_mix, gain_ffn, routes_across, weights_across) = small[7:]
    (out, new_keys, new_values, new_log_gate) = results_v
    (keys_v, values_v, logcum_v, wo_v, gate_v, up_v, down_v) = refs[38:45]
    (w_own, w_in, normed, t_in, sums, p_out, p_in) = refs[45:52]
    (query_s, own_value_s, columns_s, heads_s, own_kv) = refs[52:57]
    (mix_out, mix_in, mixed_res, packed, z_in, x_in, share_out, share_in, back_out, back_in) = refs[57:67]
    (small_sem, result_sem, load_sem, w_sem, t_sem, p_sem, pair_sem, y_sem, z_sem, x_sem, g_sem, s_sem, b_sem) = refs[67:]

    ep, y = lax.axis_index("ep"), lax.axis_index("tp")
    z = lax.div(ep, FLAT)
    at = lax.rem(ep, FLAT)
    x, c = lax.div(at, NC), lax.rem(at, NC)
    rows, width = tokens.shape
    part = width // ny
    query_cols = w_query.shape[1]
    heads = query_cols // HEAD_DIM
    stacked = rows * heads
    span = keys.shape[2]

    def chip(dz, dx):
        return lax.rem(z + dz, nz) * FLAT + lax.rem(x + dx, NX) * NC + c

    def row_peer(d):
        return z * FLAT + lax.rem(at + d, FLAT)

    def y_peer(d):
        return lax.rem(y + d, ny)

    partner = ep + 1 - 2 * c
    barrier = pltpu.get_barrier_semaphore()
    parity = lax.rem(y, 2)

    def signal(ep_to, y_to):
        pl.semaphore_signal(barrier, inc=1, device_id=(ep_to, y_to), device_id_type=MESH)

    for d in range(1, nz):
        signal(chip(d, 0), y)
    for d in range(1, FLAT):
        signal(row_peer(d), y)
    for d in range(1, ny):
        signal(ep, y_peer(d))

    fetches = [
        pltpu.make_async_copy(src, dst, small_sem.at[i]) for i, (src, dst) in enumerate(zip(small_hbm, small))
    ]
    for fetch in fetches:
        fetch.start()
    writes = [
        pltpu.make_async_copy(src, dst, result_sem.at[i])
        for i, (src, dst) in enumerate(zip(results_v, results_hbm))
    ]
    loads = [
        pltpu.make_async_copy(src, dst, load_sem.at[i])
        for i, (src, dst) in enumerate(
            (
                (keys, keys_v),
                (logcum, logcum_v),
                (values, values_v),
                (w_out, wo_v),
                (gate, gate_v.at[0]),
                (up, up_v.at[0]),
                (down, down_v.at[0]),
            )
        )
    ]
    for fetch in fetches:
        fetch.wait()

    w_own[:, :query_cols] = w_query[...]
    w_own[:, query_cols : query_cols + HEAD_DIM] = w_key[...]
    w_own[:, query_cols + HEAD_DIM :] = w_value[...]
    scaled = rms_scaled(tokens[...].astype(F32), gain_attn[...]).astype(BF16)
    slab = width // nz
    for k in range(nz):
        normed[k] = scaled[:, k * slab : (k + 1) * slab]
    pl.semaphore_wait(barrier, nz - 1 + FLAT - 1 + ny - 1)

    offsets = near_order(nz)
    far_first = offsets[:0:-1]
    w_copies = [
        remote(w_own, w_in.at[at], w_sem.at[0, d], w_sem.at[1, d], row_peer(d), y)
        for d in range(1, FLAT)
    ]
    t_copies = [
        remote(normed.at[lax.rem(z + d, nz)], t_in.at[d], t_sem.at[0, d], t_sem.at[1, d], chip(d, 0), y)
        for d in far_first
    ]
    for copy in t_copies + w_copies:
        copy.start()
    for load in loads:
        load.start()
    w_in[at] = w_own[...]
    t_in[0] = normed[z]
    log_gate = log_sigmoid(dot_across(scaled, w_forget[...]) + forget_bias[...])
    new_log_gate[...] = log_sigmoid(
        dot_across(w_forget[...], scaled) + jnp.transpose(jnp.broadcast_to(forget_bias[...], (rows, heads)))
    )
    writes[3].start()
    for copy in w_copies + t_copies:
        copy.wait_recv()
    product = dot(
        t_in[...].reshape(nz * rows, slab), w_in[...].reshape(FLAT * w_own.shape[0], w_own.shape[1])
    )
    steps = rows // TOGETHER
    for step in range(steps):
        for d in range(1, nz):
            first = d * rows + step * TOGETHER
            p_out[step, d] = product[first : first + TOGETHER].astype(BF16)
    sums[...] = product[:rows]
    p_copies = {}
    for step in range(steps):
        for d in far_first:
            p_copies[step, d] = remote(
                p_out.at[step, d],
                p_in.at[step, d],
                p_sem.at[0, step, d],
                p_sem.at[1, step, d],
                chip(nz - d, 0),
                y,
            )
            p_copies[step, d].start()
    shape = (nz * 2 * SLOTS, rows)
    lane = iota(shape, 0)
    expert_of = 2 * lax.rem(z + lane // (2 * SLOTS), nz) + (lane // SLOTS) % 2
    picking, _, _ = slotted(routes_across[0:1, :], routes_across[1:2, :], expert_of, lane % SLOTS, 1)
    picking = picking.astype(BF16)
    unit = ones_where(iota((rows, rows), 0) == iota((rows, rows), 1))
    routes = dot_across(unit, routes_across[...].astype(F32)).astype(jnp.int32)
    weights = dot_across(unit, weights_across[...], EXACT)
    shape = (rows, nz * NX * SLOTS)
    lane = iota(shape, 1)
    place = lane // (NX * SLOTS)
    dz_of = jnp.where(place % 2 == 1, (place + 1) // 2, nz - place // 2)
    expert_of = 2 * lax.rem(z + dz_of, nz) + lax.rem(x + (lane // SLOTS) % NX, NX) // 2
    weighing, in_first, in_second = slotted(routes[:, 0:1], routes[:, 1:2], expert_of, lane % SLOTS, 0)
    weighing = weighing * (
        jnp.where(in_first, weights[:, 0:1], 0.0) + jnp.where(in_second, weights[:, 1:2], 0.0)
    )
    coarse = weighing.astype(BF16)
    fine = (weighing - coarse.astype(F32)).astype(BF16)
    repeat = ones_where(iota((stacked, rows), 0) // heads == iota((stacked, rows), 1))
    gate_of = jnp.dot(repeat, log_gate, precision=EXACT, preferred_element_type=F32)
    own_head = iota((stacked, heads), 1) == iota((stacked, heads), 0) % heads
    gate_of = jnp.sum(jnp.where(own_head, gate_of, 0.0), axis=1, keepdims=True)
    fold = ones_where(iota((query_cols, HEAD_DIM), 0) % HEAD_DIM == iota((query_cols, HEAD_DIM), 1))
    fold = fold.astype(BF16)
    columns_s[:, 1:2] = gate_of
    some = TOGETHER * heads
    repeat = ones_where(iota((some, TOGETHER), 0) // heads == iota((some, TOGETHER), 1)).astype(BF16)
    gather = ones_where(iota((TOGETHER, some), 1) // heads == iota((TOGETHER, some), 0)).astype(BF16)
    own_part = iota((some, query_cols), 1) // HEAD_DIM == iota((some, query_cols), 0) % heads
    pair_copies = [
        remote(src, dst.at[1], pair_sem.at[0, i], pair_sem.at[1, i], partner, y)
        for i, (src, dst) in enumerate(((gate, gate_v), (up, up_v), (down, down_v)))
    ]

    def prepare(step):
        at_rows = slice(step * TOGETHER, (step + 1) * TOGETHER)
        at_heads = slice(step * some, (step + 1) * some)
        for d in far_first:
            p_copies[step, d].wait_recv()
        total = sums[at_rows, :]
        for d in range(1, nz):
            total = total + p_in[step, d].astype(F32)
        projected = total.astype(BF16)
        own_kv[at_rows, :] = projected[:, query_cols:].astype(F32)
        new_key = projected[:, query_cols : query_cols + HEAD_DIM]
        new_value = projected[:, query_cols + HEAD_DIM :]
        spread = jnp.where(own_part, dot(repeat, projected[:, :query_cols]), 0.0).astype(BF16)
        query_of = dot(spread, fold) * HEAD_DIM ** (-0.5)
        query_s[at_heads, :] = query_of
        columns_s[at_heads, 0:1] = jnp.sum(query_of * dot(repeat, new_key), axis=1, keepdims=True)
        own_value_s[at_heads, :] = dot(repeat, new_value)

    def attend(step):
        group = []
        for j in range(TOGETHER):
            b = step * TOGETHER + j
            at_rows = pl.ds(pl.multiple_of(b * heads, heads), heads)
            score = dot(query_s[at_rows, :].astype(BF16), keys_v[b])
            group.append((b, at_rows, score))
        for j, (b, at_rows, score) in enumerate(group):
            cum = logcum_v[b]
            length = lengths[b]
            position = iota((heads, span), 1)
            last = jnp.sum(jnp.where(position == length - 1, cum, 0.0), axis=1, keepdims=True)
            own = columns_s[at_rows, 0:1]
            shift = (last + columns_s[at_rows, 1:2]) - cum
            past = jnp.where(position < length, score + shift, MASKED)
            peak = jnp.maximum(jnp.max(past, axis=1, keepdims=True), own)
            past = jnp.exp(past - peak)
            own = jnp.exp(own - peak)
            group[j] = (b, at_rows, past, own, jnp.sum(past, axis=1, keepdims=True) + own)
        for b, at_rows, past, own, norm in group:
            mixed = dot_across(past.astype(BF16), values_v[b]) + own * own_value_s[at_rows, :]
            heads_s[at_rows, :] = mixed / norm

    y_copies = []
    for step in range(steps):
        prepare(step)
        if step == 0:
            for load in loads[:3]:
                load.wait()
        if step == steps - 1:
            for copy in pair_copies:
                copy.start()
        attend(step)
        mixed = heads_s[step * some : (step + 1) * some, :].astype(BF16)
        spread = jnp.where(own_part, dot_across(mixed, fold), 0.0).astype(BF16)
        heads_out = dot(gather, spread).astype(BF16)
        if step == 0:
            loads[3].wait()
        mix_out[step] = dot(heads_out, wo_v[...]).astype(BF16)
        for d in range(1, ny):
            copy = remote(
                mix_out.at[step],
                mix_in.at[d, step],
                y_sem.at[0, d, step],
                y_sem.at[1, d, step],
                ep,
                y_peer(d),
            )
            copy.start()
            y_copies.append(copy)
    new_keys[...] = own_kv[:, :HEAD_DIM].astype(BF16)
    new_values[...] = own_kv[:, HEAD_DIM:].astype(BF16)
    writes[1].start()
    writes[2].start()
    for copy in w_copies + t_copies + list(p_copies.values()):
        copy.wait_send()
    for load in loads[4:]:
        load.wait()
    mix = mix_out[...].reshape(rows, width).astype(F32)
    for copy in y_copies:
        copy.wait_recv()
    for d in range(1, ny):
        mix = mix + mix_in[d].reshape(rows, width).astype(F32)
    mixed = tokens[...].astype(F32) + rms_scaled(mix, gain_mix[...])
    for k in range(ny):
        mixed_res[k] = mixed[:, k * part : (k + 1) * part]
    ffn_in = rms_scaled(mixed, gain_ffn[...]).astype(BF16)
    quarters = [ffn_in[:, k * part : (k + 1) * part] for k in range(ny)]
    sides = [jnp.concatenate((quarters[k], quarters[k + 2]), axis=1) for k in range(2)]
    side = jnp.where(parity == 0, sides[0], sides[1])
    packed[...] = dot(picking, side).astype(BF16).reshape(nz, 2, SLOTS, width // 2)

    z_copies = [None] + [
        remote(packed.at[d], z_in.at[parity, p], z_sem.at[0, p], z_sem.at[1, p], chip(d, 0), y)
        for p, d in enumerate(offsets)
        if p
    ]
    for copy in z_copies[1:]:
        copy.start()
    for k in range(2):
        own = dot(picking[: 2 * SLOTS], sides[k]).astype(BF16)
        z_in[k, 0] = own.reshape(2, SLOTS, width // 2)
    x_copies, g_copies, s_copies, b_copies = {}, {}, {}, []
    chunks = CHUNKS

    def hand_over(p):
        z_copies[p].wait_recv()
        for i, d in enumerate((ny - 1, 1)):
            block = z_in.at[parity, p, i]
            g_copies[p, i] = remote(block, block, g_sem.at[0, p, i], g_sem.at[1, p, i], ep, y_peer(d))
            g_copies[p, i].start()

    def forward(p):
        if p:
            for i in range(2):
                g_copies[p, i].wait_recv()
        for dx in range(1, NX):
            half = lax.rem(x + dx, NX) // 2
            x_copies[p, dx] = remote(
                z_in.at[:, p, half], x_in.at[:, p, dx], x_sem.at[0, p, dx], x_sem.at[1, p, dx], chip(0, dx), y
            )
            x_copies[p, dx].start()
        for k in range(2):
            x_in[k, p, 0] = z_in[k, p, x // 2]

    def multiply(chunk):
        lo, hi = chunk
        for p in range(lo, hi):
            for dx in range(1, NX):
                x_copies[p, dx].wait_recv()
        if lo == 0:
            for copy in pair_copies:
                copy.wait_recv()
        count = (hi - lo) * NX * SLOTS
        first = lo * NX * SLOTS
        arrived = [x_in[k, lo:hi].reshape(count, width // 2) for k in range(2)]
        hidden = []
        for k in range(NC):
            gate_part = of_both(arrived, gate_v, k)
            up_part = of_both(arrived, up_v, k)
            hidden.append((gate_part / (1.0 + jnp.exp(-gate_part)) * up_part).astype(BF16))
        for j in range(ny):
            cols = slice(j * part, (j + 1) * part)
            share = dot(hidden[0], down_v[0, :, cols]) + dot(hidden[1], down_v[1, :, cols])
            share_out[j, first : first + count] = share.astype(BF16)
        for d in range(1, ny):
            s_copies[lo, d] = remote(
                share_out.at[y_peer(d), pl.ds(first, count)],
                share_in.at[d, pl.ds(first, count)],
                s_sem.at[0, lo, d],
                s_sem.at[1, lo, d],
                ep,
                y_peer(d),
            )
            s_copies[lo, d].start()

    def give_back(chunk):
        lo, hi = chunk
        count = (hi - lo) * NX * SLOTS
        here = pl.ds(lo * NX * SLOTS, count)
        total = share_out[y, here].astype(F32)
        for d in range(1, ny):
            s_copies[lo, d].wait_recv()
            total = total + share_in[d, here].astype(F32)
        back_out[lo:hi] = total.astype(BF16).reshape(hi - lo, NX, SLOTS, part)
        for p in range(lo, hi):
            for dx in range(NX):
                if p or dx:
                    copy = remote(
                        back_out.at[p, dx],
                        back_in.at[p, dx],
                        b_sem.at[0, p, dx],
                        b_sem.at[1, p, dx],
                        chip(nz - offsets[p], NX - dx),
                        y,
                    )
                    copy.start()
                    b_copies.append(copy)
                else:
                    back_in[0, 0] = back_out[0, 0]

    for step, argument in SCHEDULE:
        if step == "x":
            forward(argument)
        elif step == "y":
            hand_over(argument)
        elif step == "m":
            multiply(chunks[argument])
        else:
            give_back(chunks[argument])
    for copy in y_copies + pair_copies + z_copies[1:] + list(x_copies.values()):
        copy.wait_send()
    for copy in list(g_copies.values()) + list(s_copies.values()):
        copy.wait_send()
    for copy in b_copies:
        copy.wait_recv()
    returned = back_in[...].reshape(nz * NX * SLOTS, part)
    out[...] = (mixed_res[y] + (dot(coarse, returned) + dot(fine, returned))).astype(BF16)
    writes[0].start()
    for copy in b_copies:
        copy.wait_send()
    for write in writes:
        write.wait()


def write_kernel(*refs):
    for src, dst in zip(refs[:4], refs[4:]):
        dst[...] = src[...]


def body(
    nz,
    ny,
    tokens,
    norm_gain_attn,
    w_query,
    w_key,
    w_value,
    w_forget,
    forget_bias,
    cache_keys,
    cache_values,
    cache_logcum,
    lengths,
    w_out,
    norm_gain_mix,
    norm_gain_ffn,
    expert_gate,
    expert_up,
    expert_down,
    routes,
    route_weights,
):
    rows, width = tokens.shape
    part = width // ny
    query_cols = w_query.shape[1]
    cols = query_cols + w_key.shape[1] + w_value.shape[1]
    heads = query_cols // HEAD_DIM
    hidden = expert_gate.shape[1]
    depth = w_query.shape[0]
    stacked = rows * heads
    lanes = nz * NX * SLOTS
    steps = rows // TOGETHER
    vmem = pl.BlockSpec(memory_space=pltpu.VMEM)
    kept = pl.BlockSpec(memory_space=pl.ANY)
    smem = pl.BlockSpec(memory_space=pltpu.SMEM)

    def dma(*shape):
        return pltpu.SemaphoreType.DMA((2, *shape))

    small = (
        tokens,
        norm_gain_attn[None, :],
        w_query,
        w_key,
        w_value,
        w_forget.T,
        forget_bias[None, :],
        norm_gain_mix[None, :],
        norm_gain_ffn[None, :],
        routes.T,
        route_weights.T,
    )
    shapes = (
        jax.ShapeDtypeStruct((rows, part), BF16),
        jax.ShapeDtypeStruct((rows, HEAD_DIM), BF16),
        jax.ShapeDtypeStruct((rows, HEAD_DIM), BF16),
        jax.ShapeDtypeStruct((heads, rows), F32),
    )
    results = pl.pallas_call(
        functools.partial(layer_kernel, nz, ny),
        out_shape=shapes,
        in_specs=[kept] * 18 + [smem],
        out_specs=(kept,) * 4,
        scratch_shapes=[
            *(pltpu.VMEM(a.shape, a.dtype) for a in (*small, *shapes)),
            pltpu.VMEM(cache_keys.shape, BF16),
            pltpu.VMEM(cache_values.shape, BF16),
            pltpu.VMEM(cache_logcum.shape, F32),
            pltpu.VMEM(w_out.shape, BF16),
            pltpu.VMEM((NC, 2, 2, part, hidden), BF16),
            pltpu.VMEM((NC, 2, 2, part, hidden), BF16),
            pltpu.VMEM((NC, hidden, width), BF16),
            pltpu.VMEM((depth, cols), BF16),
            pltpu.VMEM((FLAT, depth, cols), BF16),
            pltpu.VMEM((nz, rows, width // nz), BF16),
            pltpu.VMEM((nz, rows, width // nz), BF16),
            pltpu.VMEM((rows, cols), F32),
            pltpu.VMEM((steps, nz, TOGETHER, cols), BF16),
            pltpu.VMEM((steps, nz, TOGETHER, cols), BF16),
            pltpu.VMEM((stacked, HEAD_DIM), F32),
            pltpu.VMEM((stacked, HEAD_DIM), F32),
            pltpu.VMEM((stacked, 2), F32),
            pltpu.VMEM((stacked, HEAD_DIM), F32),
            pltpu.VMEM((rows, 2 * HEAD_DIM), F32),
            pltpu.VMEM((steps, TOGETHER, width), BF16),
            pltpu.VMEM((ny, steps, TOGETHER, width), BF16),
            pltpu.VMEM((ny, rows, part), F32),
            pltpu.VMEM((nz, 2, SLOTS, width // 2), BF16),
            pltpu.VMEM((2, nz, 2, SLOTS, width // 2), BF16),
            pltpu.VMEM((2, nz, NX, SLOTS, width // 2), BF16),
            pltpu.VMEM((ny, lanes, part), BF16),
            pltpu.VMEM((ny, lanes, part), BF16),
            pltpu.VMEM((nz, NX, SLOTS, part), BF16),
            pltpu.VMEM((nz, NX, SLOTS, part), BF16),
            pltpu.SemaphoreType.DMA((len(small),)),
            pltpu.SemaphoreType.DMA((len(shapes),)),
            pltpu.SemaphoreType.DMA((7,)),
            dma(FLAT),
            dma(nz),
            dma(steps, nz),
            dma(3),
            dma(ny, steps),
            dma(nz),
            dma(nz, NX),
            dma(nz, 2),
            dma(nz, ny),
            dma(nz, NX),
        ],
        compiler_params=pltpu.CompilerParams(collective_id=0, has_side_effects=True),
        name="layer",
    )(
        *small,
        cache_keys,
        cache_values,
        cache_logcum,
        w_out,
        expert_gate.reshape(2, 2, part, hidden),
        expert_up.reshape(2, 2, part, hidden),
        expert_down,
        lengths,
    )
    layer_out, new_keys, new_values, new_log_gate = pl.pallas_call(
        write_kernel,
        out_shape=tuple(jax.ShapeDtypeStruct(a.shape, a.dtype) for a in results),
        in_specs=(vmem,) * 4,
        out_specs=(vmem,) * 4,
        name="write",
    )(*results)
    return layer_out, new_keys, new_values, new_log_gate.T


def solution(mesh):
    placed = (
        P("ep", None),
        P(),
        P("ep", "tp"),
        P("ep", "tp"),
        P("ep", "tp"),
        P(None, "tp"),
        P("tp"),
        P("ep", "tp", None),
        P("ep", "tp", None),
        P("ep", "tp", None),
        P("ep"),
        P("tp", None),
        P(),
        P(),
        P(None, ("ep", "tp")),
        P(None, ("ep", "tp")),
        P(("ep", "tp"), None),
        P("ep", None),
        P("ep", None),
    )
    nz = mesh.shape["ep"] // FLAT
    return jax.shard_map(
        functools.partial(body, nz, mesh.shape["tp"]),
        mesh=mesh,
        in_specs=placed,
        out_specs=(P("ep", "tp"), P("ep", "tp"), P("ep", "tp"), P("ep", "tp")),
        check_vma=False,
    )
```

```python
import functools

import jax
import jax.numpy as jnp
from jax import lax
from jax.experimental import pallas as pl
from jax.experimental.pallas import tpu as pltpu
from jax.sharding import PartitionSpec as P

HEAD_DIM = 64
NX = 4
NC = 2
FLAT = NX * NC
SLOTS = 8
TOGETHER = 8
HANDED = 8
CHUNKS = ((0, 1), (1, 3), (3, 5), (5, 7), (7, 8))
SCHEDULE = (
    *(("x", 0), ("x", 1), ("x", 2), ("m", 0), ("x", 3), ("x", 4), ("x", 5), ("x", 6), ("x", 7),),
    *(("m", 1), ("m", 2), ("m", 3), ("m", 4), ("r", 0), ("r", 1), ("r", 2), ("r", 3), ("r", 4),),
)
EPSILON = 1e-06
MASKED = -1e30
MESH = pl.DeviceIdType.MESH
F32 = jnp.float32
BF16 = jnp.bfloat16
EXACT = lax.Precision.HIGHEST
ACROSS = (((1,), (1,)), ((), ()))


def rms_scaled(field, gain_vector):
    return (
        field * lax.rsqrt(jnp.mean(field * field, axis=-1, keepdims=True) + EPSILON) * gain_vector
    )


def log_sigmoid(v):
    return jnp.minimum(v, 0.0) - jnp.log1p(jnp.exp(-jnp.abs(v)))


def dot(a, b):
    return jnp.dot(a, b, preferred_element_type=F32)


def dot_across(a, b, precision=None):
    return lax.dot_general(a, b, ACROSS, precision=precision, preferred_element_type=F32)


def iota(shape, dim):
    return lax.broadcasted_iota(jnp.int32, shape, dim)


def ones_where(mask):
    return jnp.where(mask, 1.0, 0.0).astype(F32)


def remote(src, dst, send, recv, ep, y):
    return pltpu.make_async_remote_copy(
        src_ref=src, dst_ref=dst, send_sem=send, recv_sem=recv, device_id=(ep, y), device_id_type=MESH
    )


def slotted(first, second, expert_of, slot_of, axis):
    in_first, in_second = first == expert_of, second == expert_of
    member = ones_where(in_first | in_second)
    rows = member.shape[axis]
    if axis == 0:
        before = ones_where(iota((rows, rows), 1) < iota((rows, rows), 0)).astype(BF16)
        earlier = dot(before, member.astype(BF16))
    else:
        before = ones_where(iota((rows, rows), 0) < iota((rows, rows), 1)).astype(BF16)
        earlier = dot(member.astype(BF16), before)
    return jnp.where(earlier == slot_of.astype(F32), member, 0.0), in_first, in_second


def near_order(n):
    return [(p + 1) // 2 if p % 2 else (n - p // 2) % n for p in range(n)]


def of_both(sides, weights, k):
    depth, cols = 2 * weights.shape[3], weights.shape[4]
    return sum(dot(side, weights[k, :, i].reshape(depth, cols)) for i, side in enumerate(sides))


def layer_kernel(nz, ny, *refs):
    small_hbm, (keys, values, logcum, w_out, gate, up, down), lengths = refs[:11], refs[11:18], refs[18]
    results_hbm, small, results_v = refs[19:23], refs[23:34], refs[34:38]
    (tokens, gain_attn, w_query, w_key, w_value, w_forget, forget_bias) = small[:7]
    (gain_mix, gain_ffn, routes_across, weights_across) = small[7:]
    (out, new_keys, new_values, new_log_gate) = results_v
    (keys_v, values_v, logcum_v, wo_v, gate_v, up_v, down_v) = refs[38:45]
    (w_own, w_in, normed, t_in, sums, p_out, p_in) = refs[45:52]
    (query_s, own_value_s, columns_s, heads_s, own_kv) = refs[52:57]
    (mix_out, mix_in, mixed_res, packed, z_in, x_in, share_out, share_in, back_out, back_in) = refs[57:67]
    (small_sem, result_sem, load_sem, w_sem, t_sem, p_sem, pair_sem, y_sem, z_sem, x_sem, g_sem, s_sem, b_sem) = refs[67:]

    ep, y = lax.axis_index("ep"), lax.axis_index("tp")
    z = lax.div(ep, FLAT)
    at = lax.rem(ep, FLAT)
    x, c = lax.div(at, NC), lax.rem(at, NC)
    rows, width = tokens.shape
    part = width // ny
    query_cols = w_query.shape[1]
    heads = query_cols // HEAD_DIM
    stacked = rows * heads
    span = keys.shape[2]

    def chip(dz, dx):
        return lax.rem(z + dz, nz) * FLAT + lax.rem(x + dx, NX) * NC + c

    def row_peer(d):
        return z * FLAT + lax.rem(at + d, FLAT)

    def y_peer(d):
        return lax.rem(y + d, ny)

    partner = ep + 1 - 2 * c
    barrier = pltpu.get_barrier_semaphore()
    parity = lax.rem(y, 2)

    def signal(ep_to, y_to):
        pl.semaphore_signal(barrier, inc=1, device_id=(ep_to, y_to), device_id_type=MESH)

    for d in range(1, nz):
        signal(chip(d, 0), y)
    for d in range(1, FLAT):
        signal(row_peer(d), y)
    for d in range(1, ny):
        signal(ep, y_peer(d))

    fetches = [
        pltpu.make_async_copy(src, dst, small_sem.at[i]) for i, (src, dst) in enumerate(zip(small_hbm, small))
    ]
    for fetch in fetches:
        fetch.start()
    writes = [
        pltpu.make_async_copy(src, dst, result_sem.at[i])
        for i, (src, dst) in enumerate(zip(results_v, results_hbm))
    ]
    loads = [
        pltpu.make_async_copy(src, dst, load_sem.at[i])
        for i, (src, dst) in enumerate(
            (
                (keys, keys_v),
                (logcum, logcum_v),
                (values, values_v),
                (w_out, wo_v),
                (gate, gate_v.at[0]),
                (up, up_v.at[0]),
                (down, down_v.at[0]),
            )
        )
    ]
    for fetch in fetches:
        fetch.wait()

    w_own[:, :query_cols] = w_query[...]
    w_own[:, query_cols : query_cols + HEAD_DIM] = w_key[...]
    w_own[:, query_cols + HEAD_DIM :] = w_value[...]
    scaled = rms_scaled(tokens[...].astype(F32), gain_attn[...]).astype(BF16)
    slab = width // nz
    for k in range(nz):
        normed[k] = scaled[:, k * slab : (k + 1) * slab]
    pl.semaphore_wait(barrier, nz - 1 + FLAT - 1 + ny - 1)

    offsets = near_order(nz)
    far_first = offsets[:0:-1]
    w_copies = [
        remote(w_own, w_in.at[at], w_sem.at[0, d], w_sem.at[1, d], row_peer(d), y)
        for d in range(1, FLAT)
    ]
    t_copies = [
        remote(normed.at[lax.rem(z + d, nz)], t_in.at[d], t_sem.at[0, d], t_sem.at[1, d], chip(d, 0), y)
        for d in far_first
    ]
    for copy in t_copies + w_copies:
        copy.start()
    for load in loads:
        load.start()
    w_in[at] = w_own[...]
    t_in[0] = normed[z]
    log_gate = log_sigmoid(dot_across(scaled, w_forget[...]) + forget_bias[...])
    new_log_gate[...] = log_sigmoid(
        dot_across(w_forget[...], scaled) + jnp.transpose(jnp.broadcast_to(forget_bias[...], (rows, heads)))
    )
    writes[3].start()
    for copy in w_copies + t_copies:
        copy.wait_recv()
    product = dot(
        t_in[...].reshape(nz * rows, slab), w_in[...].reshape(FLAT * w_own.shape[0], w_own.shape[1])
    )
    steps = rows // TOGETHER
    for step in range(steps):
        for d in range(1, nz):
            first = d * rows + step * TOGETHER
            p_out[step, d] = product[first : first + TOGETHER].astype(BF16)
    sums[...] = product[:rows]
    p_copies = {}
    for step in range(steps):
        for d in far_first:
            p_copies[step, d] = remote(
                p_out.at[step, d],
                p_in.at[step, d],
                p_sem.at[0, step, d],
                p_sem.at[1, step, d],
                chip(nz - d, 0),
                y,
            )
            p_copies[step, d].start()
    shape = (nz * 2 * SLOTS, rows)
    lane = iota(shape, 0)
    expert_of = 2 * lax.rem(z + lane // (2 * SLOTS), nz) + (lane // SLOTS) % 2
    picking, _, _ = slotted(routes_across[0:1, :], routes_across[1:2, :], expert_of, lane % SLOTS, 1)
    picking = picking.astype(BF16)
    unit = ones_where(iota((rows, rows), 0) == iota((rows, rows), 1))
    routes = dot_across(unit, routes_across[...].astype(F32)).astype(jnp.int32)
    weights = dot_across(unit, weights_across[...], EXACT)
    shape = (rows, nz * NX * SLOTS)
    lane = iota(shape, 1)
    place = lane // (NX * SLOTS)
    dz_of = jnp.where(place % 2 == 1, (place + 1) // 2, nz - place // 2)
    expert_of = 2 * lax.rem(z + dz_of, nz) + lax.rem(x + (lane // SLOTS) % NX, NX) // 2
    weighing, in_first, in_second = slotted(routes[:, 0:1], routes[:, 1:2], expert_of, lane % SLOTS, 0)
    weighing = weighing * (
        jnp.where(in_first, weights[:, 0:1], 0.0) + jnp.where(in_second, weights[:, 1:2], 0.0)
    )
    coarse = weighing.astype(BF16)
    fine = (weighing - coarse.astype(F32)).astype(BF16)
    repeat = ones_where(iota((stacked, rows), 0) // heads == iota((stacked, rows), 1))
    gate_of = jnp.dot(repeat, log_gate, precision=EXACT, preferred_element_type=F32)
    own_head = iota((stacked, heads), 1) == iota((stacked, heads), 0) % heads
    gate_of = jnp.sum(jnp.where(own_head, gate_of, 0.0), axis=1, keepdims=True)
    fold = ones_where(iota((query_cols, HEAD_DIM), 0) % HEAD_DIM == iota((query_cols, HEAD_DIM), 1))
    fold = fold.astype(BF16)
    columns_s[:, 1:2] = gate_of
    some = TOGETHER * heads
    repeat = ones_where(iota((some, TOGETHER), 0) // heads == iota((some, TOGETHER), 1)).astype(BF16)
    gather = ones_where(iota((TOGETHER, some), 1) // heads == iota((TOGETHER, some), 0)).astype(BF16)
    own_part = iota((some, query_cols), 1) // HEAD_DIM == iota((some, query_cols), 0) % heads
    pair_copies = [
        remote(src, dst.at[1], pair_sem.at[0, i], pair_sem.at[1, i], partner, y)
        for i, (src, dst) in enumerate(((gate, gate_v), (up, up_v), (down, down_v)))
    ]

    def prepare(step):
        at_rows = slice(step * TOGETHER, (step + 1) * TOGETHER)
        at_heads = slice(step * some, (step + 1) * some)
        for d in far_first:
            p_copies[step, d].wait_recv()
        total = sums[at_rows, :]
        for d in range(1, nz):
            total = total + p_in[step, d].astype(F32)
        projected = total.astype(BF16)
        own_kv[at_rows, :] = projected[:, query_cols:].astype(F32)
        new_key = projected[:, query_cols : query_cols + HEAD_DIM]
        new_value = projected[:, query_cols + HEAD_DIM :]
        spread = jnp.where(own_part, dot(repeat, projected[:, :query_cols]), 0.0).astype(BF16)
        query_of = dot(spread, fold) * HEAD_DIM ** (-0.5)
        query_s[at_heads, :] = query_of
        columns_s[at_heads, 0:1] = jnp.sum(query_of * dot(repeat, new_key), axis=1, keepdims=True)
        own_value_s[at_heads, :] = dot(repeat, new_value)

    def attend(step):
        group = []
        for j in range(TOGETHER):
            b = step * TOGETHER + j
            at_rows = pl.ds(pl.multiple_of(b * heads, heads), heads)
            score = dot(query_s[at_rows, :].astype(BF16), keys_v[b])
            group.append((b, at_rows, score))
        for j, (b, at_rows, score) in enumerate(group):
            cum = logcum_v[b]
            length = lengths[b]
            position = iota((heads, span), 1)
            last = jnp.sum(jnp.where(position == length - 1, cum, 0.0), axis=1, keepdims=True)
            own = columns_s[at_rows, 0:1]
            shift = (last + columns_s[at_rows, 1:2]) - cum
            past = jnp.where(position < length, score + shift, MASKED)
            peak = jnp.maximum(jnp.max(past, axis=1, keepdims=True), own)
            past = jnp.exp(past - peak)
            own = jnp.exp(own - peak)
            group[j] = (b, at_rows, past, own, jnp.sum(past, axis=1, keepdims=True) + own)
        for b, at_rows, past, own, norm in group:
            mixed = dot_across(past.astype(BF16), values_v[b]) + own * own_value_s[at_rows, :]
            heads_s[at_rows, :] = mixed / norm

    y_copies = []
    for step in range(steps):
        prepare(step)
        if step == 0:
            for load in loads[:3]:
                load.wait()
        if step == steps - 1:
            for copy in pair_copies:
                copy.start()
        attend(step)
        mixed = heads_s[step * some : (step + 1) * some, :].astype(BF16)
        spread = jnp.where(own_part, dot_across(mixed, fold), 0.0).astype(BF16)
        heads_out = dot(gather, spread).astype(BF16)
        if step == 0:
            loads[3].wait()
        mix_out[step] = dot(heads_out, wo_v[...]).astype(BF16)
        for d in range(1, ny):
            copy = remote(
                mix_out.at[step],
                mix_in.at[d, step],
                y_sem.at[0, d, step],
                y_sem.at[1, d, step],
                ep,
                y_peer(d),
            )
            copy.start()
            y_copies.append(copy)
    new_keys[...] = own_kv[:, :HEAD_DIM].astype(BF16)
    new_values[...] = own_kv[:, HEAD_DIM:].astype(BF16)
    writes[1].start()
    writes[2].start()
    for copy in w_copies + t_copies + list(p_copies.values()):
        copy.wait_send()
    for load in loads[4:]:
        load.wait()
    mix = mix_out[...].reshape(rows, width).astype(F32)
    for copy in y_copies:
        copy.wait_recv()
    for d in range(1, ny):
        mix = mix + mix_in[d].reshape(rows, width).astype(F32)
    mixed = tokens[...].astype(F32) + rms_scaled(mix, gain_mix[...])
    for k in range(ny):
        mixed_res[k] = mixed[:, k * part : (k + 1) * part]
    ffn_in = rms_scaled(mixed, gain_ffn[...]).astype(BF16)
    quarters = [ffn_in[:, k * part : (k + 1) * part] for k in range(ny)]
    sides = [jnp.concatenate((quarters[k], quarters[k + 2]), axis=1) for k in range(2)]
    for k in range(2):
        packed[k] = dot(picking, sides[k]).astype(BF16).reshape(nz, 2, SLOTS, width // 2)

    z_copies = [None]
    for p, d in enumerate(offsets):
        if p:
            kind = slice(None) if p < HANDED else parity
            copy = remote(
                packed.at[kind, d], z_in.at[kind, p], z_sem.at[0, p], z_sem.at[1, p], chip(d, 0), y
            )
            z_copies.append(copy)
    for copy in z_copies[1:]:
        copy.start()
    for k in range(2):
        z_in[k, 0] = packed[k, 0]
    x_copies, g_copies, s_copies, b_copies = {}, {}, {}, []
    chunks = CHUNKS

    def hand_over(p):
        z_copies[p].wait_recv()
        for i, d in enumerate((ny - 1, 1)):
            block = z_in.at[parity, p, i]
            g_copies[p, i] = remote(block, block, g_sem.at[0, p, i], g_sem.at[1, p, i], ep, y_peer(d))
            g_copies[p, i].start()

    def forward(p):
        if p >= HANDED:
            for i in range(2):
                g_copies[p, i].wait_recv()
        elif p:
            z_copies[p].wait_recv()
        for dx in range(1, NX):
            half = lax.rem(x + dx, NX) // 2
            x_copies[p, dx] = remote(
                z_in.at[:, p, half], x_in.at[:, p, dx], x_sem.at[0, p, dx], x_sem.at[1, p, dx], chip(0, dx), y
            )
            x_copies[p, dx].start()
        for k in range(2):
            x_in[k, p, 0] = z_in[k, p, x // 2]

    def multiply(chunk):
        lo, hi = chunk
        for p in range(lo, hi):
            for dx in range(1, NX):
                x_copies[p, dx].wait_recv()
        if lo == 0:
            for copy in pair_copies:
                copy.wait_recv()
        count = (hi - lo) * NX * SLOTS
        first = lo * NX * SLOTS
        arrived = [x_in[k, lo:hi].reshape(count, width // 2) for k in range(2)]
        hidden = []
        for k in range(NC):
            gate_part = of_both(arrived, gate_v, k)
            up_part = of_both(arrived, up_v, k)
            hidden.append((gate_part / (1.0 + jnp.exp(-gate_part)) * up_part).astype(BF16))
        for j in range(ny):
            cols = slice(j * part, (j + 1) * part)
            share = dot(hidden[0], down_v[0, :, cols]) + dot(hidden[1], down_v[1, :, cols])
            share_out[j, first : first + count] = share.astype(BF16)
        for d in range(1, ny):
            s_copies[lo, d] = remote(
                share_out.at[y_peer(d), pl.ds(first, count)],
                share_in.at[d, pl.ds(first, count)],
                s_sem.at[0, lo, d],
                s_sem.at[1, lo, d],
                ep,
                y_peer(d),
            )
            s_copies[lo, d].start()

    def give_back(chunk):
        lo, hi = chunk
        count = (hi - lo) * NX * SLOTS
        here = pl.ds(lo * NX * SLOTS, count)
        total = share_out[y, here].astype(F32)
        for d in range(1, ny):
            s_copies[lo, d].wait_recv()
            total = total + share_in[d, here].astype(F32)
        back_out[lo:hi] = total.astype(BF16).reshape(hi - lo, NX, SLOTS, part)
        for p in range(lo, hi):
            for dx in range(NX):
                if p or dx:
                    copy = remote(
                        back_out.at[p, dx],
                        back_in.at[p, dx],
                        b_sem.at[0, p, dx],
                        b_sem.at[1, p, dx],
                        chip(nz - offsets[p], NX - dx),
                        y,
                    )
                    copy.start()
                    b_copies.append(copy)
                else:
                    back_in[0, 0] = back_out[0, 0]

    for step, argument in SCHEDULE:
        if step == "x":
            forward(argument)
        elif step == "y":
            hand_over(argument)
        elif step == "m":
            multiply(chunks[argument])
        else:
            give_back(chunks[argument])
    for copy in y_copies + pair_copies + z_copies[1:] + list(x_copies.values()):
        copy.wait_send()
    for copy in list(g_copies.values()) + list(s_copies.values()):
        copy.wait_send()
    for copy in b_copies:
        copy.wait_recv()
    returned = back_in[...].reshape(nz * NX * SLOTS, part)
    out[...] = (mixed_res[y] + (dot(coarse, returned) + dot(fine, returned))).astype(BF16)
    writes[0].start()
    for copy in b_copies:
        copy.wait_send()
    for write in writes:
        write.wait()


def write_kernel(*refs):
    for src, dst in zip(refs[:4], refs[4:]):
        dst[...] = src[...]


def body(
    nz,
    ny,
    tokens,
    norm_gain_attn,
    w_query,
    w_key,
    w_value,
    w_forget,
    forget_bias,
    cache_keys,
    cache_values,
    cache_logcum,
    lengths,
    w_out,
    norm_gain_mix,
    norm_gain_ffn,
    expert_gate,
    expert_up,
    expert_down,
    routes,
    route_weights,
):
    rows, width = tokens.shape
    part = width // ny
    query_cols = w_query.shape[1]
    cols = query_cols + w_key.shape[1] + w_value.shape[1]
    heads = query_cols // HEAD_DIM
    hidden = expert_gate.shape[1]
    depth = w_query.shape[0]
    stacked = rows * heads
    lanes = nz * NX * SLOTS
    steps = rows // TOGETHER
    vmem = pl.BlockSpec(memory_space=pltpu.VMEM)
    kept = pl.BlockSpec(memory_space=pl.ANY)
    smem = pl.BlockSpec(memory_space=pltpu.SMEM)

    def dma(*shape):
        return pltpu.SemaphoreType.DMA((2, *shape))

    small = (
        tokens,
        norm_gain_attn[None, :],
        w_query,
        w_key,
        w_value,
        w_forget.T,
        forget_bias[None, :],
        norm_gain_mix[None, :],
        norm_gain_ffn[None, :],
        routes.T,
        route_weights.T,
    )
    shapes = (
        jax.ShapeDtypeStruct((rows, part), BF16),
        jax.ShapeDtypeStruct((rows, HEAD_DIM), BF16),
        jax.ShapeDtypeStruct((rows, HEAD_DIM), BF16),
        jax.ShapeDtypeStruct((heads, rows), F32),
    )
    results = pl.pallas_call(
        functools.partial(layer_kernel, nz, ny),
        out_shape=shapes,
        in_specs=[kept] * 18 + [smem],
        out_specs=(kept,) * 4,
        scratch_shapes=[
            *(pltpu.VMEM(a.shape, a.dtype) for a in (*small, *shapes)),
            pltpu.VMEM(cache_keys.shape, BF16),
            pltpu.VMEM(cache_values.shape, BF16),
            pltpu.VMEM(cache_logcum.shape, F32),
            pltpu.VMEM(w_out.shape, BF16),
            pltpu.VMEM((NC, 2, 2, part, hidden), BF16),
            pltpu.VMEM((NC, 2, 2, part, hidden), BF16),
            pltpu.VMEM((NC, hidden, width), BF16),
            pltpu.VMEM((depth, cols), BF16),
            pltpu.VMEM((FLAT, depth, cols), BF16),
            pltpu.VMEM((nz, rows, width // nz), BF16),
            pltpu.VMEM((nz, rows, width // nz), BF16),
            pltpu.VMEM((rows, cols), F32),
            pltpu.VMEM((steps, nz, TOGETHER, cols), BF16),
            pltpu.VMEM((steps, nz, TOGETHER, cols), BF16),
            pltpu.VMEM((stacked, HEAD_DIM), F32),
            pltpu.VMEM((stacked, HEAD_DIM), F32),
            pltpu.VMEM((stacked, 2), F32),
            pltpu.VMEM((stacked, HEAD_DIM), F32),
            pltpu.VMEM((rows, 2 * HEAD_DIM), F32),
            pltpu.VMEM((steps, TOGETHER, width), BF16),
            pltpu.VMEM((ny, steps, TOGETHER, width), BF16),
            pltpu.VMEM((ny, rows, part), F32),
            pltpu.VMEM((2, nz, 2, SLOTS, width // 2), BF16),
            pltpu.VMEM((2, nz, 2, SLOTS, width // 2), BF16),
            pltpu.VMEM((2, nz, NX, SLOTS, width // 2), BF16),
            pltpu.VMEM((ny, lanes, part), BF16),
            pltpu.VMEM((ny, lanes, part), BF16),
            pltpu.VMEM((nz, NX, SLOTS, part), BF16),
            pltpu.VMEM((nz, NX, SLOTS, part), BF16),
            pltpu.SemaphoreType.DMA((len(small),)),
            pltpu.SemaphoreType.DMA((len(shapes),)),
            pltpu.SemaphoreType.DMA((7,)),
            dma(FLAT),
            dma(nz),
            dma(steps, nz),
            dma(3),
            dma(ny, steps),
            dma(nz),
            dma(nz, NX),
            dma(nz, 2),
            dma(nz, ny),
            dma(nz, NX),
        ],
        compiler_params=pltpu.CompilerParams(collective_id=0, has_side_effects=True),
        name="layer",
    )(
        *small,
        cache_keys,
        cache_values,
        cache_logcum,
        w_out,
        expert_gate.reshape(2, 2, part, hidden),
        expert_up.reshape(2, 2, part, hidden),
        expert_down,
        lengths,
    )
    layer_out, new_keys, new_values, new_log_gate = pl.pallas_call(
        write_kernel,
        out_shape=tuple(jax.ShapeDtypeStruct(a.shape, a.dtype) for a in results),
        in_specs=(vmem,) * 4,
        out_specs=(vmem,) * 4,
        name="write",
    )(*results)
    return layer_out, new_keys, new_values, new_log_gate.T


def solution(mesh):
    placed = (
        P("ep", None),
        P(),
        P("ep", "tp"),
        P("ep", "tp"),
        P("ep", "tp"),
        P(None, "tp"),
        P("tp"),
        P("ep", "tp", None),
        P("ep", "tp", None),
        P("ep", "tp", None),
        P("ep"),
        P("tp", None),
        P(),
        P(),
        P(None, ("ep", "tp")),
        P(None, ("ep", "tp")),
        P(("ep", "tp"), None),
        P("ep", None),
        P("ep", None),
    )
    nz = mesh.shape["ep"] // FLAT
    return jax.shard_map(
        functools.partial(body, nz, mesh.shape["tp"]),
        mesh=mesh,
        in_specs=placed,
        out_specs=(P("ep", "tp"), P("ep", "tp"), P("ep", "tp"), P("ep", "tp")),
        check_vma=False,
    )
```
